32 devices in a mesh: st: 4 (over y, x), tp: 8 (over z, core).
Axes of the slice: x: 2, y: 2, z: 4, core: 2. Of those that a mesh axis runs over, the one named last changes fastest.
Arguments:
- tokens: bfloat16 [2048, 4096], P('st', 'tp'), may hold values from -6 to 6
- w_query: bfloat16 [4096, 2048], P(None, 'tp'), may hold values from -0.09375 to 0.09375
- w_key: bfloat16 [4096, 2048], P(None, 'tp'), may hold values from -0.09375 to 0.09375
- w_value: bfloat16 [4096, 4096], P(None, 'tp'), may hold values from -0.09375 to 0.09375
- w_mem_query: bfloat16 [4096, 2048], P(None, 'tp'), may hold values from -0.09375 to 0.09375
- w_mem_key: bfloat16 [4096, 2048], P(None, 'tp'), may hold values from -0.09375 to 0.09375
- w_mem_value: bfloat16 [4096, 2048], P(None, 'tp'), may hold values from -0.09375 to 0.09375
- w_gate: bfloat16 [4096, 16], P(None, 'tp'), may hold values from -0.09375 to 0.09375
- w_lift: bfloat16 [16, 128, 256], P('tp'), may hold values from -4 to 4
- decay_rate: float32 [16], P('tp'), may hold values from 0.000390625 to 0.1
- store: bfloat16 [512, 64, 4096], P('st', None, 'tp'), may hold values from -6 to 6
- passage_ids: int32 [16, 2], P('st'), may hold values from 0 to 511, as said below
Outputs:
- mixed: bfloat16 [2048, 4096], P('st', 'tp')
The draws below stay inside these ranges and needn't reach their ends.
Inputs may be any that keep to these rules, and one draw needn't show every extreme that they name: `passage_ids`: passage p is held by index p // 128 of st. Among the requests of the rows of one device along st, at most 4 name passages held by one index of st, and in every draw some index receives exactly 4 of them.
All inputs are finite; a program needn't handle non-finite values.
Results may differ from the reference program's by a relative error of at most 0.0095.
Values may be sent and summed in bfloat16 or wider, within the bound.
A program may use at most 64 MiB of HBM per device.

```python
import jax
import jax.numpy as jnp
from jax import lax

D = 4096
HEADS = 16
KEY_DIM = 128
VALUE_DIM = 256
MEM_DIM = 128
TOK_DEV = 512
SEQ_LEN = 512
RET_BLOCK = 64
BLOCK = 128
PICKS = 2
PASS_ROWS = 64
PASS_DEV = 128
CAP = 4
TOKENS = 2048
BLOCKS = 16
PASSAGES = 512
N_ST = 4


def draw_decay_rate(key, part):
    pick_key, slow_key, fast_key = jax.random.split(key, 3)
    quick = jax.random.uniform(pick_key, (HEADS,)) < 0.5
    slow_rate = jnp.exp(jax.random.uniform(slow_key, (HEADS,), minval=jnp.log(0.2 / SEQ_LEN), maxval=jnp.log(2.0 / SEQ_LEN)))
    fast_rate = jnp.exp(jax.random.uniform(fast_key, (HEADS,), minval=jnp.log(0.03), maxval=jnp.log(0.1)))
    return jnp.where(quick, fast_rate, slow_rate).astype(jnp.float32)


def draw_passage_ids(key, part):
    requests = TOK_DEV // BLOCK * PICKS
    slot_count = N_ST * CAP
    owners = jnp.repeat(jnp.arange(N_ST, dtype=jnp.int32), CAP)
    copies = jnp.tile(jnp.arange(CAP, dtype=jnp.int32), N_ST)

    def one_device(device):
        device_key = jax.random.fold_in(key, device)
        rank_key, shuffle_key, first_key, second_key = jax.random.split(device_key, 4)
        before = (device + N_ST - 1) % N_ST
        across = (device + N_ST // 2) % N_ST
        priority = jnp.where(owners == before, 0, jnp.where((owners == across) & (copies == 0), 1, 2))
        noise_rank = jax.random.randint(rank_key, (slot_count,), 0, 1 << 12)
        scores = priority * (1 << 24) + noise_rank * slot_count + jnp.arange(slot_count, dtype=jnp.int32)
        chosen = owners[jnp.argsort(scores)[:requests]]
        chosen = chosen[jax.random.permutation(shuffle_key, requests)]
        first_pick = jax.random.randint(first_key, (requests,), 0, PASS_DEV)
        second_pick = jax.random.randint(second_key, (requests,), 0, PASS_DEV)
        return chosen * PASS_DEV + jnp.minimum(first_pick, second_pick)
    drawn = jax.vmap(one_device)(jnp.arange(N_ST, dtype=jnp.int32))
    return drawn.reshape(BLOCKS, PICKS).astype(jnp.int32)


def block_scale(stream_key, extent, cuts, least, top_value):
    def one(dim, shards_of):
        heights = jax.random.uniform(jax.random.fold_in(jax.random.fold_in(stream_key, 6), dim), (shards_of,), jnp.float32, least / len(cuts), top_value / len(cuts))
        return jnp.repeat(jnp.exp(heights), extent[dim] // shards_of).reshape((-1,) + (1,) * (len(extent) - dim - 1))

    factor_of = one(*cuts[0])
    for cut in cuts[1:]:
        factor_of = factor_of * one(*cut)
    return factor_of


def noise(key, dims, scale, limit, cuts=(), held_as=jnp.bfloat16):
    entries = scale * jax.random.normal(key, dims, jnp.float32)
    if cuts:
        entries = entries * block_scale(key, dims, cuts, -0.22, 0.18)
    return jnp.clip(entries, -limit, limit).astype(held_as)


def setup_inputs(seed: int = 0) -> dict:
    streams_of = jax.random.split(jax.random.key(seed), 13)
    return {
        "tokens": noise(streams_of[0], (TOKENS, D), 1.0, 6.0, ((0, 4), (1, 8))),
        "w_query": noise(streams_of[1], (D, HEADS * KEY_DIM), D ** -0.5, 0.09375, ((1, 8),)),
        "w_key": noise(streams_of[2], (D, HEADS * KEY_DIM), D ** -0.5, 0.09375, ((1, 8),)),
        "w_value": noise(streams_of[3], (D, HEADS * VALUE_DIM), D ** -0.5, 0.09375, ((1, 8),)),
        "w_mem_query": noise(streams_of[4], (D, HEADS * MEM_DIM), D ** -0.5, 0.09375, ((1, 8),)),
        "w_mem_key": noise(streams_of[5], (D, HEADS * MEM_DIM), D ** -0.5, 0.09375, ((1, 8),)),
        "w_mem_value": noise(streams_of[6], (D, HEADS * MEM_DIM), D ** -0.5, 0.09375, ((1, 8),)),
        "w_gate": noise(streams_of[7], (D, HEADS), D ** -0.5, 0.09375, ((1, 8),)),
        "w_lift": noise(streams_of[8], (HEADS, MEM_DIM, VALUE_DIM), 0.7, 4.0, ((0, 8),)),
        "decay_rate": draw_decay_rate(jax.random.fold_in(streams_of[12], 71), 0),
        "store": noise(streams_of[10], (PASSAGES, PASS_ROWS, D), 1.0, 6.0, ((0, 4), (2, 8))),
        "passage_ids": draw_passage_ids(jax.random.fold_in(streams_of[12], 71), 0),
    }


norm_eps = 1e-06
rope_base = 10000.0

def rotate(values, positions):
    half_dim = values.shape[-1] // 2
    inverse = rope_base ** (-jnp.arange(half_dim, dtype=jnp.float32) / half_dim)
    angles = positions.astype(jnp.float32)[:, None] * inverse[None, :]
    cosine = jnp.cos(angles)[:, None, :]
    sine_table = jnp.sin(angles)[:, None, :]
    first_half = values[..., :half_dim]
    second_half = values[..., half_dim:]
    return jnp.concatenate([first_half * cosine - second_half * sine_table, first_half * sine_table + second_half * cosine], axis=-1)

def head_norm(values):
    return values * lax.rsqrt(lax.optimization_barrier(jnp.mean(values * values, axis=-1, keepdims=True)) + norm_eps)

def group_norm(values):
    centred = values - lax.optimization_barrier(jnp.mean(values, axis=-1, keepdims=True))
    return centred * lax.rsqrt(lax.optimization_barrier(jnp.mean(centred * centred, axis=-1, keepdims=True)) + norm_eps)

def retention(ret_query, ret_key, ret_value, rates, block_len):
    tokens_all, head_count, key_dim = ret_query.shape
    value_dim = ret_value.shape[-1]
    sequences = tokens_all // SEQ_LEN
    block_count = SEQ_LEN // block_len

    def blocked(array):
        shaped = array.astype(jnp.float32).reshape(sequences, block_count, block_len, head_count, array.shape[-1])
        return jnp.swapaxes(shaped, 0, 1)
    log_decay = -rates.astype(jnp.float32)
    offsets = jnp.arange(block_len, dtype=jnp.float32)
    decay_query = jnp.exp(log_decay[None, :] * (offsets[:, None] + 1.0))
    distance = offsets[:, None] - offsets[None, :]
    decay_mask = jnp.where(distance[None] >= 0.0, jnp.exp(log_decay[:, None, None] * jnp.maximum(distance, 0.0)[None]), 0.0)
    decay_key = jnp.exp(log_decay[None, :] * (block_len - 1.0 - offsets[:, None]))
    decay_block = jnp.exp(log_decay * block_len)
    highest = lax.Precision.HIGHEST

    def advance(memory_state, pieces):
        query_block, key_block, value_block = pieces
        carried = jnp.einsum('slhk,shkv->slhv', query_block, memory_state, precision=highest) * decay_query[None, :, :, None]
        scores = jnp.einsum('slhk,smhk->shlm', query_block, key_block, precision=highest) * decay_mask[None]
        within = jnp.einsum('shlm,smhv->slhv', scores, value_block, precision=highest)
        weighted = key_block * decay_key[None, :, :, None]
        memory_state = decay_block[None, :, None, None] * memory_state + jnp.einsum('slhk,slhv->shkv', weighted, value_block, precision=highest)
        return (memory_state, carried + within)
    initial = jnp.zeros((sequences, head_count, key_dim, value_dim), jnp.float32)
    _, outputs = lax.scan(advance, initial, (blocked(ret_query), blocked(ret_key), blocked(ret_value)))
    return jnp.swapaxes(outputs, 0, 1).reshape(tokens_all, head_count, value_dim)

def reference(tokens, w_query, w_key, w_value, w_mem_query, w_mem_key, w_mem_value, w_gate, w_lift, decay_rate, store, passage_ids):
    total_rows = tokens.shape[0]
    head_count = decay_rate.shape[0]
    highest = lax.Precision.HIGHEST
    features = tokens.astype(jnp.float32)
    row_scale = lax.rsqrt(lax.optimization_barrier(jnp.mean(features * features, axis=1, keepdims=True)) + norm_eps)
    positions = jnp.arange(total_rows, dtype=jnp.int32) % SEQ_LEN

    def project(weight):
        return jnp.dot(tokens, weight, preferred_element_type=jnp.float32)
    ret_query = rotate((project(w_query) * row_scale).reshape(total_rows, head_count, KEY_DIM), positions).astype(jnp.bfloat16)
    ret_key = (rotate((project(w_key) * row_scale).reshape(total_rows, head_count, KEY_DIM), positions) * KEY_DIM ** (-0.5)).astype(jnp.bfloat16)
    ret_value = (project(w_value) * row_scale).astype(jnp.bfloat16).reshape(total_rows, head_count, VALUE_DIM)
    mem_query = head_norm(project(w_mem_query).reshape(total_rows, head_count, MEM_DIM)).astype(jnp.bfloat16)
    gate_value = jax.nn.sigmoid(project(w_gate) * row_scale)
    ret_norm = group_norm(retention(ret_query, ret_key, ret_value, decay_rate, RET_BLOCK))

    def passage_rows(ident):
        passage = lax.dynamic_index_in_dim(store, ident, 0, keepdims=False)
        key_part = head_norm(jnp.dot(passage, w_mem_key, preferred_element_type=jnp.float32).reshape(PASS_ROWS, head_count, MEM_DIM))
        value_part = jnp.dot(passage, w_mem_value, preferred_element_type=jnp.float32).reshape(PASS_ROWS, head_count, MEM_DIM)
        return (key_part.astype(jnp.bfloat16), value_part.astype(jnp.bfloat16))
    pass_key, pass_value = lax.map(passage_rows, passage_ids.reshape(-1).astype(jnp.int32))
    block_count, picks = passage_ids.shape
    query_blocks = mem_query.reshape(block_count, BLOCK, head_count, MEM_DIM)
    key_blocks = pass_key.reshape(block_count, picks, PASS_ROWS, head_count, MEM_DIM)
    value_blocks = pass_value.reshape(block_count, picks, PASS_ROWS, head_count, MEM_DIM)

    def attend(pieces):
        query_block, key_block, value_block = pieces
        scores = jnp.einsum('thd,prhd->hptr', query_block.astype(jnp.float32), key_block.astype(jnp.float32), precision=highest) * MEM_DIM ** (-0.5)
        exponent = jnp.exp(scores)
        mass_sum = lax.optimization_barrier(jnp.sum(exponent, axis=3))
        rounded = lax.optimization_barrier(exponent.astype(jnp.bfloat16)).astype(jnp.float32)
        partial_value = jnp.einsum('hptr,prhd->pthd', rounded, value_block.astype(jnp.float32), precision=highest)
        partial_value = lax.optimization_barrier(partial_value.astype(jnp.bfloat16)).astype(jnp.float32)
        summed = lax.optimization_barrier(jnp.sum(partial_value, axis=0))
        return summed / jnp.swapaxes(lax.optimization_barrier(jnp.sum(mass_sum, axis=1)), 0, 1)[:, :, None]
    mem_out = lax.map(attend, (query_blocks, key_blocks, value_blocks)).reshape(total_rows, head_count, MEM_DIM).astype(jnp.bfloat16)
    mem_lift = jnp.einsum('thd,hde->the', mem_out.astype(jnp.float32), w_lift.astype(jnp.float32), precision=highest)
    mixed = (ret_norm + gate_value[:, :, None] * mem_lift).astype(jnp.bfloat16)
    return mixed.reshape(total_rows, head_count * VALUE_DIM)
```

```python
import functools

import jax
import jax.numpy as jnp
import numpy as np
from jax import lax
from jax.experimental import pallas as pl
from jax.experimental.pallas import tpu as pltpu
from jax.sharding import PartitionSpec as P

KEY_DIM = 128
VALUE_DIM = 256
MEM_DIM = 128
SEQ_LEN = 512
NORM_EPS = 1e-06
ROPE_BASE = 10000.0
CORES = 2
PIECES = 4
OUT, IN = 0, 1
MESH = pl.DeviceIdType.MESH
F32 = jnp.float32
BF16 = jnp.bfloat16


def dot(a, b):
    return jnp.dot(a, b, preferred_element_type=F32)


def dot_nt(a, b):
    return lax.dot_general(a, b, (((1,), (1,)), ((), ())), preferred_element_type=F32)


def square_split(n):
    return 1 << ((n.bit_length() - 1) // 2)


def kernel(
    n_st, n_tp, cap, picks, held,
    rate_ref, tok_hbm, wq_hbm, wk_hbm, wv_hbm, wm_hbm, wmk_hbm, wmv_hbm, wg_ref, lift_hbm,
    cos_hbm, sin_hbm, store_hbm, ids_hbm,
    out_ref,
    tok, rows, cos_ref, sin_ref, lift_ref, wq, wk, wv, wm, wmk, wmv, store, slots, landed, ids_v, ids_s,
    acc_q, acc_k, acc_v, acc_m, acc_g, acc_s, acc_mk, acc_mv,
    rq, rk, rv, mq, ret, gate, xwk, xwv, kv_out, kv_in,
    load_sem, id_send, id_recv, pass_send, pass_recv,
    t_sems, r_sems, w_send, w_recv, spread_send, kv_send, kv_recv,
):
    st = lax.axis_index("st")
    me = lax.axis_index("tp")
    z = me // CORES
    core = me % CORES
    n_z = n_tp // CORES
    total, cols = tok.shape[1:]
    heads = mq.shape[1] // MEM_DIM
    mem_cols = mq.shape[1]
    requests = ids_s.shape[1] * ids_s.shape[2]
    blocks = requests // picks
    pass_rows = store.shape[1]
    parts = len(landed)
    per = cap // parts
    chunk = total // PIECES
    rows_piece = rows.shape[1] // PIECES

    so = jnp.where(z < n_z // 2, -1, 1)
    depth = jnp.minimum(z, n_z - 1 - z)
    edge_z = z + so * depth
    is_edge = depth == 0
    is_helper = depth == 1
    me_out = me + CORES * so
    me_in = me - CORES * so
    pair = me + 1 - 2 * core
    outs = range(1, (n_z - 1) // 2 + 1)
    ins = range(1, n_z)

    loads = []
    pairs = [(store_hbm, store), (ids_hbm, ids_v.at[st]), (tok_hbm, tok.at[me]), (wq_hbm, wq), (wk_hbm, wk),
             (wv_hbm, wv), (wm_hbm, wm), (wmk_hbm, wmk), (wmv_hbm, wmv),
             (cos_hbm, cos_ref), (sin_hbm, sin_ref), (lift_hbm, lift_ref)]
    for i, (src, dst) in enumerate(pairs):
        loads.append(pltpu.make_async_copy(src, dst, load_sem.at[i]))
    loads[1].start()

    barrier = pltpu.get_barrier_semaphore()

    def greet(to_st, to_tp):
        pl.semaphore_signal(barrier, inc=1, device_id=(to_st, to_tp), device_id_type=MESH)

    @pl.when(depth > 0)
    def _():
        greet(st, me_out)
    greet(st, me_in)
    greet(st, pair)
    for d in range(1, n_st):
        greet((st + d) % n_st, me)
    pl.semaphore_wait(barrier, n_st + 1 + (depth > 0).astype(jnp.int32))

    def remote(src, dst, send, recv, to_st, to_tp):
        return pltpu.make_async_remote_copy(
            src_ref=src, dst_ref=dst, send_sem=send, recv_sem=recv,
            device_id=(to_st, to_tp), device_id_type=MESH)

    class Flow:
        def __init__(self, buf, sems, floor, source=None):
            self.buf, self.floor, self.source = buf, floor, source
            self.recv, self.send, self.own_out, self.pairing = sems
            self.size = buf.shape[1] // PIECES

        def piece(self, j, p):
            return self.buf.at[j, pl.ds(p * self.size, self.size)]

        def origin(self, p):
            return self.piece(me, p) if self.source is None else self.source.at[pl.ds(p * self.size, self.size)]

        def copy(self, j, p, sem, to, src=None):
            return remote(self.piece(j, p) if src is None else src, self.piece(j, p), sem, self.recv.at[j, p], st, to)

        def to_in(self, j, p, src=None):
            return self.copy(j, p, self.send.at[j, p], me_in, src)

        def to_out(self, j, p, src=None):
            return self.copy(j, p, self.send.at[j, p] if src is None else self.own_out.at[p], me_out, src)

        def to_pair(self, j, p, src=None):
            return self.copy(j, p, self.pairing.at[j, p], pair, src)

        def send_own(self, p):
            self.to_in(me, p, self.origin(p)).start()

            @pl.when(depth > self.floor)
            def _():
                self.to_out(me, p, self.origin(p)).start()

        def share_own(self, p):
            self.to_pair(me, p, self.origin(p)).start()

        def at(self, side, d):
            far = CORES * so * d
            if side == OUT:
                return me + far, d <= depth
            return me - far, (d <= n_z - 1 - depth) & (depth >= self.floor)

        def relay(self, side, d, p):
            j, valid = self.at(side, d)

            @pl.when(valid)
            def _():
                self.to_pair(j, p).wait_recv()
                if side == OUT:
                    self.to_in(j, p).start()
                else:
                    @pl.when(depth > self.floor)
                    def _():
                        self.to_out(j, p).start()
                self.to_pair(j, p).start()

        def consume(self, side, d, first, last, take):
            j, valid = self.at(side, d)

            def step(q, carry):
                p, which = first + q // CORES, q % CORES
                this = j + which * (1 - 2 * core)

                @pl.when(which == 1)
                def _():
                    self.to_pair(this, p).wait_recv()
                take(this, p)
                return carry

            if d == 0:
                lax.fori_loop(0, CORES * (last - first), step, 0)
            else:
                @pl.when(valid)
                def _():
                    lax.fori_loop(0, CORES * (last - first), step, 0)

        def drain(self):
            def step(p, carry):
                self.to_in(me, p, self.origin(p)).wait_send()
                self.to_pair(me, p, self.origin(p)).wait_send()

                @pl.when(depth > self.floor)
                def _():
                    self.to_out(me, p, self.origin(p)).wait_send()
                for side, distances in ((OUT, outs), (IN, ins)):
                    for d in distances:
                        j, valid = self.at(side, d)

                        @pl.when(valid)
                        def _():
                            if side == OUT:
                                self.to_in(j, p).wait_send()
                            else:
                                @pl.when(depth > self.floor)
                                def _():
                                    self.to_out(j, p).wait_send()
                            self.to_pair(j, p).wait_send()
                return carry
            lax.fori_loop(0, PIECES, step, 0)

    toks = Flow(tok, t_sems, 0, tok_hbm)
    passes = Flow(rows, r_sems, 1)

    n_b = square_split(n_st)
    n_a = n_st // n_b
    a, b = st // n_b, st % n_b
    row_mates = [a * n_b + (b + i) % n_b for i in range(1, n_b)]
    col_mates = [(a + i) % n_a * n_b + b for i in range(1, n_a)]
    mates = row_mates + col_mates
    along_row = range(0, n_b - 1)
    along_col = range(n_b - 1, len(mates))
    sub = CORES * cols // n_st
    lent = 2 * (n_z - 1)
    xw = (xwk, xwv)

    def lent_at(e, s):
        return pl.ds(pl.multiple_of((edge_z - so * (e + 1)) * (CORES * cols) + s * sub, sub), sub)

    def lend(w):
        kv, e = w % 2, w // 2
        at = lent_at(e, st)
        return remote((wmk_hbm, wmv_hbm)[kv].at[at], xw[kv].at[at], w_send.at[kv, e], w_recv.at[kv, e, st], st, me_in)

    def spread(kv, e, s, i):
        here = xw[kv].at[lent_at(e, s)]
        return remote(here, here, spread_send.at[kv, i, s], w_recv.at[kv, e, s], mates[i], me)

    def spread_own(w):
        kv, e = w % 2, w // 2

        @pl.when(is_helper)
        def _():
            spread(kv, e, st, 0).wait_recv()
            for i in range(len(mates)):
                spread(kv, e, st, i).start()

    def spread_on(w):
        kv, e = w % 2, w // 2

        @pl.when(is_helper)
        def _():
            for s in (row_mates, col_mates)[kv]:
                spread(kv, e, s, 0).wait_recv()
                for i in (along_col, along_row)[kv]:
                    spread(kv, e, s, i).start()

    def spread_last(w):
        kv, e = w % 2, w // 2

        @pl.when(is_helper)
        def _():
            if kv == 0:
                rest = [(a + i) % n_a * n_b + k for i in range(1, n_a) for k in range(n_b)]
            else:
                rest = [k * n_b + (b + i) % n_b for i in range(1, n_b) for k in range(n_a)]
            for s in rest:
                spread(kv, e, s, 0).wait_recv()

    def spread_drain():
        def all_of(kv, s, i):
            whole = xw[kv].at[pl.ds(0, (n_z - 1) * sub)]
            return remote(whole, whole, spread_send.at[kv, i, s], w_recv.at[kv, 0, s], mates[i], me)

        @pl.when(is_helper)
        def _():
            for kv in range(2):
                for i in range(len(mates)):
                    all_of(kv, st, i).wait_send()
                for s in (row_mates, col_mates)[kv]:
                    for i in (along_col, along_row)[kv]:
                        all_of(kv, s, i).wait_send()

        @pl.when(is_edge)
        def _():
            for w in range(lent):
                lend(w).wait_send()

    def kv_copy(p):
        at = pl.ds(p * rows_piece, rows_piece)
        return remote(kv_out.at[at], kv_in.at[at], kv_send.at[p], kv_recv.at[p], st, me_out)

    def id_copy(d):
        return remote(ids_hbm, ids_v.at[st], id_send.at[d], id_recv.at[st], (st + d) % n_st, me)

    def id_wait(d):
        other = (st + d) % n_st
        return remote(ids_hbm, ids_v.at[other], id_send.at[d], id_recv.at[other], other, me)

    half = PIECES // 2
    late = lent - 2
    for d in range(1, n_st):
        id_copy(d).start()
    for p in range(half):
        @pl.when(is_edge)
        def _():
            lend(p).start()
        toks.send_own(p)

    @pl.when(is_edge)
    def _():
        for w in range(half, late):
            lend(w).start()

    @pl.when(depth > 0)
    def _():
        for p in range(half, PIECES):
            toks.send_own(p)
    loads[0].start()
    for p in range(PIECES):
        toks.share_own(p)
    loads[2].start()

    for ref in (acc_q, acc_k, acc_v, acc_m, acc_g, acc_s, acc_mk, acc_mv):
        ref[...] = jnp.zeros_like(ref)

    loads[1].wait()
    for d in range(1, n_st):
        id_wait(d).wait_recv()
    to_scalar = pltpu.make_async_copy(ids_v, ids_s, load_sem.at[len(pairs)])
    to_scalar.start()
    to_scalar.wait()
    loads[0].wait()

    def asked(source, k):
        found = jnp.int32(0)
        seen = jnp.int32(0)
        for i in range(requests):
            ident = ids_s[source, i % picks, i // picks]
            mine = (ident // held) == st
            found = jnp.where(mine & (seen == k), ident % held, found)
            seen = seen + mine.astype(jnp.int32)
        return found

    def pass_copy(g, d):
        return remote(slots.at[d, pl.ds(g * per, per)], landed[g].at[st], pass_send.at[g, d], pass_recv.at[g, st],
                      (st + d) % n_st, me)

    def pass_wait(g, d):
        other = (st + d) % n_st
        return remote(slots.at[d, pl.ds(g * per, per)], landed[g].at[other], pass_send.at[g, d],
                      pass_recv.at[g, other], other, me)

    for g in range(parts):
        def fill(d, carry):
            for k in range(g * per, (g + 1) * per):
                slots[d, k] = store[asked((st + d) % n_st, k)]
            return carry
        lax.fori_loop(1, n_st, fill, 0)
        for d in range(1, n_st):
            pass_copy(g, d).start()
    for k in range(cap):
        landed[k // per][st, k % per] = store[asked(st, k)]
    for i in range(3, len(pairs)):
        loads[i].start()

    def build(block):
        reach = min(parts, -(-picks * (block + 1) // per))
        for i in range(block * picks, (block + 1) * picks):
            ident = ids_s[st, i % picks, i // picks]
            owner = ident // held
            order = jnp.int32(0)
            for e in range(i):
                order = order + ((ids_s[st, e % picks, e // picks] // held) == owner).astype(jnp.int32)
            value = landed[0][owner, jnp.minimum(order, per - 1)]
            for g in range(1, reach):
                other = landed[g][owner, jnp.clip(order - g * per, 0, per - 1)]
                value = jnp.where(order >= g * per, other, value)
            rows[me, pl.ds(i * pass_rows, pass_rows), :] = value

    def build_piece(p):
        for block in range(p * blocks // PIECES, (p + 1) * blocks // PIECES):
            build(block)

    def take_tokens(j, p):
        at = pl.ds(pl.multiple_of(j * cols, cols), cols)
        here = pl.ds(pl.multiple_of(p * chunk, chunk), chunk)
        x = tok[j, here, :]
        acc_q[here, :] += dot(x, wq[at, :])
        acc_k[here, :] += dot(x, wk[at, :])
        acc_v[here, :] += dot(x, wv[at, :])
        acc_m[here, :] += dot(x, wm[at, :])
        wide = x.astype(F32)
        if heads > 1:
            acc_g[here, :] += dot_nt(x, wg_ref[:, at])
        else:
            acc_g[here, :] += jnp.sum(wide * wg_ref[:, at].astype(F32), axis=1, keepdims=True)
        squares = acc_s[here, :]
        for piece in range(cols // 128):
            slab = wide[:, piece * 128:(piece + 1) * 128]
            squares = squares + slab * slab
        acc_s[here, :] = squares

    def take_rows(j, p):
        at = pl.ds(pl.multiple_of(j * cols, cols), cols)
        here = pl.ds(pl.multiple_of(p * rows_piece, rows_piece), rows_piece)
        x = rows[j, here, :]
        acc_mk[here, :] += dot(x, wmk[at, :])
        acc_mv[here, :] += dot(x, wmv[at, :])

    def prepare(c, carry):
        here = pl.ds(pl.multiple_of(c * chunk, chunk), chunk)
        scale = lax.rsqrt(jnp.sum(acc_s[here, :], axis=1, keepdims=True) / (n_tp * cols) + NORM_EPS)
        cosine, sine = cos_ref[here, :], sin_ref[here, :]

        def rotate(v):
            return v * cosine + pltpu.roll(v, KEY_DIM // 2, 1) * sine
        for h in range(heads):
            at = slice(h * KEY_DIM, (h + 1) * KEY_DIM)
            rq[here, at] = rotate(acc_q[here, at] * scale).astype(BF16)
            rk[here, at] = (rotate(acc_k[here, at] * scale) * KEY_DIM ** (-0.5)).astype(BF16)
            m = acc_m[here, at]
            mq[here, at] = (m * lax.rsqrt(jnp.mean(m * m, axis=1, keepdims=True) + NORM_EPS)).astype(BF16)
        rv[here, :] = (acc_v[here, :] * scale).astype(BF16)
        gate[here, :] = jax.nn.sigmoid(acc_g[here, :] * scale)
        return carry

    def retain(c):
        here = pl.ds(c * chunk, chunk)
        start = (c * chunk) // SEQ_LEN * SEQ_LEN
        length = (c + 1) * chunk - start
        whole = pl.ds(start, length)
        t = lax.broadcasted_iota(jnp.int32, (chunk, length), 0) + (c * chunk - start)
        s = lax.broadcasted_iota(jnp.int32, (chunk, length), 1)
        gap = (t - s).astype(F32)
        for h in range(heads):
            at = slice(h * KEY_DIM, (h + 1) * KEY_DIM)
            wide = slice(h * VALUE_DIM, (h + 1) * VALUE_DIM)
            decay = jnp.where(gap >= 0.0, jnp.exp(-rate_ref[h] * jnp.maximum(gap, 0.0)), 0.0)
            scores = dot_nt(rq[here, at], rk[whole, at]) * decay
            upper = scores.astype(BF16)
            lower = (scores - upper.astype(F32)).astype(BF16)
            value = rv[whole, wide]
            o = dot(upper, value) + dot(lower, value)
            o = o - jnp.mean(o, axis=1, keepdims=True)
            ret[here, wide] = o * lax.rsqrt(jnp.mean(o * o, axis=1, keepdims=True) + NORM_EPS)

    def assist(p):
        @pl.when(is_helper)
        def _():
            at = pl.ds(pl.multiple_of(p * rows_piece, rows_piece), rows_piece)
            base = jnp.where(so < 0, CORES, 0)
            for kv in range(2):
                total_kv = None
                for q in range(CORES * (n_z - 1)):
                    j = base + q
                    part = dot(rows[j, at, :], xw[kv][pl.ds(pl.multiple_of(j * cols, cols), cols), :])
                    total_kv = part if total_kv is None else total_kv + part
                kv_out[at, kv * mem_cols:(kv + 1) * mem_cols] = total_kv.astype(BF16)
            kv_copy(p).start()

    block = total // blocks
    keys = picks * pass_rows

    def attend(n, carry):
        here = pl.ds(pl.multiple_of(n * block, block), block)
        there = pl.ds(pl.multiple_of(n * keys, keys), keys)
        for h in range(heads):
            at = slice(h * MEM_DIM, (h + 1) * MEM_DIM)
            wide = slice(h * VALUE_DIM, (h + 1) * VALUE_DIM)
            k = acc_mk[there, at]
            k = (k * lax.rsqrt(jnp.mean(k * k, axis=1, keepdims=True) + NORM_EPS)).astype(BF16)
            v = acc_mv[there, at].astype(BF16)
            exponent = jnp.exp(dot_nt(mq[here, at], k) * MEM_DIM ** (-0.5))
            mass = jnp.sum(exponent, axis=1, keepdims=True)
            o = (dot(exponent.astype(BF16), v) / mass).astype(BF16)
            lifted = dot(o, lift_ref[h])
            out_ref[here, wide] = (ret[here, wide] + gate[here, h:h + 1] * lifted).astype(BF16)
        return carry

    def tokens_of(side, d, first, last):
        toks.consume(side, d, first, last, take_tokens)

    def rows_of(side, d, p):
        passes.consume(side, d, p, p + 1, take_rows)

    for p in range(half):
        toks.relay(IN, 1, p)
        spread_own(p)
        for d in outs:
            toks.relay(OUT, d, p)
    for i in range(2, len(pairs)):
        loads[i].wait()
    tokens_of(IN, 0, 0, PIECES)
    for p in range(half, PIECES):
        toks.relay(IN, 1, p)

    for d in range(1, n_st):
        pass_wait(0, d).wait_recv()
    first_needs = min(parts, -(-picks * (blocks // PIECES) // per))
    for g in range(1, first_needs):
        for d in range(1, n_st):
            pass_wait(g, d).wait_recv()
    build_piece(0)
    passes.send_own(0)
    passes.share_own(0)

    @pl.when(is_edge)
    def _():
        for p in range(half, PIECES):
            toks.send_own(p)
        for w in range(late, lent):
            lend(w).start()

    tokens_of(IN, 1, 0, PIECES)
    for w in range(half, late):
        spread_own(w)
    for p in range(half):
        toks.relay(IN, 2, p)
    for d in outs:
        tokens_of(OUT, d, 0, half)
    tokens_of(IN, 2, 0, half)

    for g in range(first_needs, parts):
        for d in range(1, n_st):
            pass_wait(g, d).wait_recv()
    for p in range(1, PIECES):
        build_piece(p)
        passes.share_own(p)
    passes.send_own(1)

    @pl.when(is_edge)
    def _():
        for p in range(2, PIECES):
            passes.send_own(p)

    for d in outs:
        passes.relay(OUT, d, 0)
    passes.relay(IN, 1, 0)
    for w in range(half):
        spread_on(w)
    for p in range(half, PIECES):
        for d in outs:
            toks.relay(OUT, d, p)

    @pl.when(depth > 0)
    def _():
        for p in range(2, PIECES):
            passes.send_own(p)

    for d in ins[1:]:
        passes.relay(IN, d, 0)
    for p in range(half, PIECES):
        toks.relay(IN, 2, p)
    for d in ins[2:]:
        for p in range(half):
            toks.relay(IN, d, p)
        tokens_of(IN, d, 0, half)
    for c in range(half):
        prepare(c, 0)
        retain(c)
    for w in range(half, late):
        spread_on(w)
    for w in range(late, lent):
        spread_own(w)
    for d in outs:
        tokens_of(OUT, d, half, PIECES)
    tokens_of(IN, 2, half, PIECES)
    for d in ins[2:]:
        for p in range(half, PIECES):
            toks.relay(IN, d, p)
        tokens_of(IN, d, half, PIECES)

    def rows_relay(p):
        for d in outs:
            passes.relay(OUT, d, p)
        for d in ins:
            passes.relay(IN, d, p)

    def rows_take(p):
        rows_of(IN, 0, p)
        for d in outs:
            rows_of(OUT, d, p)
        for d in ins:
            rows_of(IN, d, p)

    rows_relay(1)
    for w in range(late, lent):
        spread_on(w)
    for c in range(half, PIECES):
        prepare(c, 0)
        retain(c)
    for w in range(lent):
        spread_last(w)

    def finish(p, carry):
        @pl.when(p > 1)
        def _():
            rows_relay(p)
        rows_take(p)
        assist(p)

        @pl.when(is_edge)
        def _():
            at = pl.ds(pl.multiple_of(p * rows_piece, rows_piece), rows_piece)
            kv_copy(p).wait_recv()
            acc_mk[at, :] += kv_in[at, :mem_cols].astype(F32)
            acc_mv[at, :] += kv_in[at, mem_cols:].astype(F32)
        share = blocks // PIECES
        lax.fori_loop(p * share, (p + 1) * share, attend, 0)
        return carry
    lax.fori_loop(0, PIECES, finish, 0)

    for d in range(1, n_st):
        id_copy(d).wait_send()
        for g in range(parts):
            pass_copy(g, d).wait_send()
    toks.drain()
    passes.drain()
    spread_drain()

    @pl.when(is_helper)
    def _():
        for p in range(PIECES):
            kv_copy(p).wait_send()


def rotary_tables(total):
    half = KEY_DIM // 2
    angle = (np.arange(total) % SEQ_LEN)[:, None] * ROPE_BASE ** (-np.arange(half) / half)[None, :]
    cosine, sine = np.cos(angle), np.sin(angle)
    return (np.concatenate([cosine, cosine], 1).astype(np.float32),
            np.concatenate([-sine, sine], 1).astype(np.float32))


def solution(mesh):
    n_st, n_tp = mesh.shape["st"], mesh.shape["tp"]
    n_z = n_tp // CORES
    assert n_z >= 4

    def per_device(tokens, w_query, w_key, w_value, w_mem_query, w_mem_key, w_mem_value, w_gate, w_lift,
                   decay_rate, store, passage_ids):
        total, cols = tokens.shape
        heads = decay_rate.shape[0]
        blocks, picks = passage_ids.shape
        requests = blocks * picks
        held, pass_rows, _ = store.shape
        cap = max(1, 2 * requests // n_st)
        parts = cap // picks if cap % picks == 0 else 1
        cosine, sine = rotary_tables(total)
        hbm = pl.BlockSpec(memory_space=pl.ANY)
        vmem = pl.BlockSpec(memory_space=pltpu.VMEM)
        smem = pl.BlockSpec(memory_space=pltpu.SMEM)
        V = pltpu.VMEM
        dma = pltpu.SemaphoreType.DMA
        wide = w_value.shape[1]
        key_cols, mem_cols = w_query.shape[1], w_mem_query.shape[1]
        n_b = square_split(n_st)
        n_mates = n_b - 1 + n_st // n_b - 1

        def flow_sems():
            return dma((n_tp, PIECES)), dma((n_tp, PIECES)), dma((PIECES,)), dma((n_tp, PIECES))
        all_rows = requests * pass_rows
        scratch = [
            V((n_tp, total, cols), BF16), V((n_tp, all_rows, cols), BF16),
            V(cosine.shape, F32), V(sine.shape, F32), V(w_lift.shape, BF16),
            V(w_query.shape, BF16), V(w_key.shape, BF16), V(w_value.shape, BF16),
            V(w_mem_query.shape, BF16), V(w_mem_key.shape, BF16), V(w_mem_value.shape, BF16),
            V(store.shape, BF16), V((n_st, cap, pass_rows, cols), BF16),
            tuple(V((n_st, cap // parts, pass_rows, cols), BF16) for _ in range(parts)),
            V((n_st, picks, blocks), jnp.int32), pltpu.SMEM((n_st, picks, blocks), jnp.int32),
            V((total, key_cols), F32), V((total, key_cols), F32), V((total, wide), F32), V((total, mem_cols), F32),
            V((total, heads), F32), V((total, 128), F32),
            V((all_rows, mem_cols), F32), V((all_rows, mem_cols), F32),
            V((total, key_cols), BF16), V((total, key_cols), BF16), V((total, wide), BF16), V((total, mem_cols), BF16),
            V((total, wide), F32), V((total, heads), F32),
            V(w_mem_key.shape, BF16), V(w_mem_value.shape, BF16),
            V((all_rows, 2 * mem_cols), BF16), V((all_rows, 2 * mem_cols), BF16),
            dma((16,)), dma((n_st,)), dma((n_st,)), dma((parts, n_st)), dma((parts, n_st)),
            flow_sems(), flow_sems(),
            dma((2, n_z - 1)), dma((2, n_z - 1, n_st)), dma((2, n_mates, n_st)), dma((PIECES,)), dma((PIECES,)),
        ]
        return pl.pallas_call(
            functools.partial(kernel, n_st, n_tp, cap, picks, held),
            out_shape=jax.ShapeDtypeStruct((total, heads * VALUE_DIM), BF16),
            in_specs=[smem] + [hbm] * 7 + [vmem] + [hbm] * 5,
            out_specs=vmem,
            scratch_shapes=scratch,
            compiler_params=pltpu.CompilerParams(
                collective_id=0, has_side_effects=True, vmem_limit_bytes=60 * 1024 * 1024),
        )(decay_rate, tokens, w_query, w_key, w_value, w_mem_query, w_mem_key, w_mem_value,
          w_gate.T, w_lift, jnp.asarray(cosine), jnp.asarray(sine), store, passage_ids.T)

    in_specs = (P("st", "tp"),) + (P(None, "tp"),) * 7 + (
        P("tp", None, None), P("tp"), P("st", None, "tp"), P("st", None))
    return jax.shard_map(per_device, mesh=mesh, in_specs=in_specs, out_specs=P("st", "tp"), check_vma=False)
```

```python
import functools

import jax
import jax.numpy as jnp
import numpy as np
from jax import lax
from jax.experimental import pallas as pl
from jax.experimental.pallas import tpu as pltpu
from jax.sharding import PartitionSpec as P

KEY_DIM = 128
VALUE_DIM = 256
MEM_DIM = 128
SEQ_LEN = 512
NORM_EPS = 1e-06
ROPE_BASE = 10000.0
CORES = 2
PIECES = 4
OUT, IN = 0, 1
MESH = pl.DeviceIdType.MESH
F32 = jnp.float32
BF16 = jnp.bfloat16


def dot(a, b):
    return jnp.dot(a, b, preferred_element_type=F32)


def dot_nt(a, b):
    return lax.dot_general(a, b, (((1,), (1,)), ((), ())), preferred_element_type=F32)


def square_split(n):
    return 1 << ((n.bit_length() - 1) // 2)


def kernel(
    n_st, n_tp, cap, picks, held,
    rate_ref, tok_hbm, wq_hbm, wk_hbm, wv_hbm, wm_hbm, wmk_hbm, wmv_hbm, wg_ref, lift_hbm,
    cos_hbm, sin_hbm, store_hbm, ids_hbm,
    out_ref,
    tok, rows, cos_ref, sin_ref, lift_ref, wq, wk, wv, wm, wmk, wmv, store, slots, landed, ids_v, ids_s,
    acc_q, acc_k, acc_v, acc_m, acc_g, acc_s, acc_mk, acc_mv,
    rq, rk, rv, mq, ret, gate, xwk, xwv, kv_out, kv_in,
    load_sem, id_send, id_recv, pass_send, pass_recv,
    t_sems, r_sems, w_send, w_recv, spread_send, kv_send, kv_recv,
):
    st = lax.axis_index("st")
    me = lax.axis_index("tp")
    z = me // CORES
    core = me % CORES
    n_z = n_tp // CORES
    total, cols = tok.shape[1:]
    heads = mq.shape[1] // MEM_DIM
    mem_cols = mq.shape[1]
    requests = ids_s.shape[1] * ids_s.shape[2]
    blocks = requests // picks
    pass_rows = store.shape[1]
    parts = len(landed)
    per = cap // parts
    chunk = total // PIECES
    rows_piece = rows.shape[1] // PIECES

    so = jnp.where(z < n_z // 2, -1, 1)
    depth = jnp.minimum(z, n_z - 1 - z)
    edge_z = z + so * depth
    is_edge = depth == 0
    is_helper = depth == 1
    me_out = me + CORES * so
    me_in = me - CORES * so
    pair = me + 1 - 2 * core
    outs = range(1, (n_z - 1) // 2 + 1)
    ins = range(1, n_z)

    loads = []
    pairs = [(store_hbm, store), (ids_hbm, ids_v.at[st]), (tok_hbm, tok.at[me]), (wq_hbm, wq), (wk_hbm, wk),
             (wv_hbm, wv), (wm_hbm, wm), (wmk_hbm, wmk), (wmv_hbm, wmv),
             (cos_hbm, cos_ref), (sin_hbm, sin_ref), (lift_hbm, lift_ref)]
    for i, (src, dst) in enumerate(pairs):
        loads.append(pltpu.make_async_copy(src, dst, load_sem.at[i]))
    loads[1].start()
    loads[0].start()
    loads[1].wait()

    barrier = pltpu.get_barrier_semaphore()

    def greet(to_st, to_tp):
        pl.semaphore_signal(barrier, inc=1, device_id=(to_st, to_tp), device_id_type=MESH)

    @pl.when(depth > 0)
    def _():
        greet(st, me_out)
    greet(st, me_in)
    greet(st, pair)
    for d in range(1, n_st):
        greet((st + d) % n_st, me)
    pl.semaphore_wait(barrier, n_st + 1 + (depth > 0).astype(jnp.int32))

    def remote(src, dst, send, recv, to_st, to_tp):
        return pltpu.make_async_remote_copy(
            src_ref=src, dst_ref=dst, send_sem=send, recv_sem=recv,
            device_id=(to_st, to_tp), device_id_type=MESH)

    class Flow:
        def __init__(self, buf, sems, floor, source=None):
            self.buf, self.floor, self.source = buf, floor, source
            self.recv, self.send, self.own_out, self.pairing = sems
            self.size = buf.shape[1] // PIECES

        def piece(self, j, p):
            return self.buf.at[j, pl.ds(p * self.size, self.size)]

        def origin(self, p):
            return self.piece(me, p) if self.source is None else self.source.at[pl.ds(p * self.size, self.size)]

        def copy(self, j, p, sem, to, src=None):
            return remote(self.piece(j, p) if src is None else src, self.piece(j, p), sem, self.recv.at[j, p], st, to)

        def to_in(self, j, p, src=None):
            return self.copy(j, p, self.send.at[j, p], me_in, src)

        def to_out(self, j, p, src=None):
            return self.copy(j, p, self.send.at[j, p] if src is None else self.own_out.at[p], me_out, src)

        def to_pair(self, j, p, src=None):
            return self.copy(j, p, self.pairing.at[j, p], pair, src)

        def send_own(self, p):
            self.to_in(me, p, self.origin(p)).start()

            @pl.when(depth > self.floor)
            def _():
                self.to_out(me, p, self.origin(p)).start()

        def share_own(self, p):
            self.to_pair(me, p, self.origin(p)).start()

        def at(self, side, d):
            far = CORES * so * d
            if side == OUT:
                return me + far, d <= depth
            return me - far, (d <= n_z - 1 - depth) & (depth >= self.floor)

        def relay(self, side, d, p):
            j, valid = self.at(side, d)

            @pl.when(valid)
            def _():
                self.to_pair(j, p).wait_recv()
                if side == OUT:
                    self.to_in(j, p).start()
                else:
                    @pl.when(depth > self.floor)
                    def _():
                        self.to_out(j, p).start()
                self.to_pair(j, p).start()

        def wait_pair(self, j, p):
            self.to_pair(j + 1 - 2 * core, p).wait_recv()

        def drain(self):
            def step(p, carry):
                self.to_in(me, p, self.origin(p)).wait_send()
                self.to_pair(me, p, self.origin(p)).wait_send()

                @pl.when(depth > self.floor)
                def _():
                    self.to_out(me, p, self.origin(p)).wait_send()
                for side, distances in ((OUT, outs), (IN, ins)):
                    for d in distances:
                        j, valid = self.at(side, d)

                        @pl.when(valid)
                        def _():
                            if side == OUT:
                                self.to_in(j, p).wait_send()
                            else:
                                @pl.when(depth > self.floor)
                                def _():
                                    self.to_out(j, p).wait_send()
                            self.to_pair(j, p).wait_send()
                return carry
            lax.fori_loop(0, PIECES, step, 0)

    toks = Flow(tok, t_sems, 0, tok_hbm)
    passes = Flow(rows, r_sems, 1)

    n_b = square_split(n_st)
    n_a = n_st // n_b
    a, b = st // n_b, st % n_b
    row_mates = [a * n_b + (b + i) % n_b for i in range(1, n_b)]
    col_mates = [(a + i) % n_a * n_b + b for i in range(1, n_a)]
    mates = row_mates + col_mates
    along_row = range(0, n_b - 1)
    along_col = range(n_b - 1, len(mates))
    sub = CORES * cols // n_st // 2
    others = n_z - 1
    lent = 2 * others
    late = lent - 2
    xw = (xwk, xwv)

    def lent_at(e, half, s):
        start = (edge_z - so * (e + 1)) * (CORES * cols) + (2 * s + half) * sub
        return pl.ds(pl.multiple_of(start, sub), sub)

    def lend(w, half):
        kv, e = w // others, w % others
        at = lent_at(e, half, st)
        return remote((wmk_hbm, wmv_hbm)[kv].at[at], xw[kv].at[at], w_send.at[kv, e, half],
                      w_recv.at[kv, e, half, st], st, me_in)

    def lend_all(first, last):
        for w in range(first, last):
            for half in range(2):
                lend(w, half).start()

    def spread(w, half, s, i):
        kv, e = w // others, w % others
        here = xw[kv].at[lent_at(e, half, s)]
        return remote(here, here, spread_send.at[kv, i, s], w_recv.at[kv, e, half, s], mates[i], me)

    def spread_own(first, last):
        @pl.when(is_helper)
        def _():
            for w in range(first, last):
                for half in range(2):
                    spread(w, half, st, 0).wait_recv()
                    for i in range(len(mates)):
                        spread(w, half, st, i).start()

    def spread_on(first, last):
        @pl.when(is_helper)
        def _():
            for w in range(first, last):
                for half in range(2):
                    for s in (row_mates, col_mates)[half]:
                        spread(w, half, s, 0).wait_recv()
                        for i in (along_col, along_row)[half]:
                            spread(w, half, s, i).start()

    def spread_last(kv):
        rest = ([(a + i) % n_a * n_b + k for i in range(1, n_a) for k in range(n_b)],
                [k * n_b + (b + i) % n_b for i in range(1, n_b) for k in range(n_a)])

        @pl.when(is_helper)
        def _():
            for w in range(kv * others, (kv + 1) * others):
                for half in range(2):
                    for s in rest[half]:
                        spread(w, half, s, 0).wait_recv()

    def spread_drain():
        def all_of(kv, s, i, halves):
            whole = xw[kv].at[pl.ds(0, others * sub * halves)]
            return remote(whole, whole, spread_send.at[kv, i, s], w_recv.at[kv, 0, 0, s], mates[i], me)

        for kv in range(2):
            for i in range(len(mates)):
                all_of(kv, st, i, 2).wait_send()
            for half in range(2):
                for s in (row_mates, col_mates)[half]:
                    for i in (along_col, along_row)[half]:
                        all_of(kv, s, i, 1).wait_send()

    def kv_copy(kv, p):
        at = pl.ds(pl.multiple_of(p * rows_piece, rows_piece), rows_piece)
        return remote(kv_out.at[kv, at], kv_in.at[kv, at], kv_send.at[kv, p], kv_recv.at[kv, p], st, me_out)

    def id_copy(d):
        return remote(ids_v.at[st], ids_v.at[st], id_send.at[d], id_recv.at[st], (st + d) % n_st, me)

    def id_wait(d):
        other = (st + d) % n_st
        return remote(ids_v.at[other], ids_v.at[other], id_send.at[d], id_recv.at[other], other, me)

    half = PIECES // 2
    for d in range(1, n_st):
        id_copy(d).start()

    @pl.when(is_edge)
    def _():
        for p in range(half):
            lend_all(p, p + 1)
            toks.send_own(p)
        lend_all(half, late)

    @pl.when(depth > 0)
    def _():
        for p in range(PIECES):
            toks.send_own(p)
    for p in range(PIECES):
        toks.share_own(p)
    loads[2].start()

    for ref in (acc_q, acc_k, acc_v, acc_m, acc_g, acc_s):
        ref[...] = jnp.zeros_like(ref)

    for d in range(1, n_st):
        id_wait(d).wait_recv()
    to_scalar = pltpu.make_async_copy(ids_v, ids_s, load_sem.at[len(pairs)])
    to_scalar.start()
    to_scalar.wait()
    loads[0].wait()
    for i in range(3, len(pairs)):
        loads[i].start()

    def asked(source, k):
        found = jnp.int32(0)
        seen = jnp.int32(0)
        for i in range(requests):
            ident = ids_s[source, i % picks, i // picks]
            mine = (ident // held) == st
            found = jnp.where(mine & (seen == k), ident % held, found)
            seen = seen + mine.astype(jnp.int32)
        return found

    def pass_copy(g, d):
        return remote(slots.at[d, pl.ds(g * per, per)], landed[g].at[st], pass_send.at[g, d], pass_recv.at[g, st],
                      (st + d) % n_st, me)

    def pass_wait(g, d):
        other = (st + d) % n_st
        return remote(slots.at[d, pl.ds(g * per, per)], landed[g].at[other], pass_send.at[g, d],
                      pass_recv.at[g, other], other, me)

    for g in range(parts):
        def fill(d, carry):
            for k in range(g * per, (g + 1) * per):
                slots[d, k] = store[asked((st + d) % n_st, k)]
            return carry
        lax.fori_loop(1, n_st, fill, 0)
        for d in range(1, n_st):
            pass_copy(g, d).start()
    for k in range(cap):
        landed[k // per][st, k % per] = store[asked(st, k)]

    def build(block):
        reach = min(parts, -(-picks * (block + 1) // per))
        for i in range(block * picks, (block + 1) * picks):
            ident = ids_s[st, i % picks, i // picks]
            owner = ident // held
            order = jnp.int32(0)
            for e in range(i):
                order = order + ((ids_s[st, e % picks, e // picks] // held) == owner).astype(jnp.int32)
            value = landed[0][owner, jnp.minimum(order, per - 1)]
            for g in range(1, reach):
                other = landed[g][owner, jnp.clip(order - g * per, 0, per - 1)]
                value = jnp.where(order >= g * per, other, value)
            rows[me, pl.ds(i * pass_rows, pass_rows), :] = value

    def build_piece(p):
        for block in range(p * blocks // PIECES, (p + 1) * blocks // PIECES):
            build(block)

    def take_tokens(at_z, h):
        here = pl.ds(pl.multiple_of(h * (half * chunk), half * chunk), half * chunk)
        xs, ats = [], []
        for c in range(CORES):
            j = at_z * CORES + c
            xs.append(tok[j, here, :])
            ats.append(pl.ds(pl.multiple_of(j * cols, cols), cols))
        for acc, w in ((acc_q, wq), (acc_k, wk), (acc_v, wv), (acc_m, wm)):
            acc[here, :] += sum(dot(x, w[at, :]) for x, at in zip(xs, ats))
        squares = acc_s[here, :]
        for x, at in zip(xs, ats):
            wide = x.astype(F32)
            if heads > 1:
                acc_g[here, :] += dot_nt(x, wg_ref[:, at])
            else:
                acc_g[here, :] += jnp.sum(wide * wg_ref[:, at].astype(F32), axis=1, keepdims=True)
            for piece in range(cols // 128):
                slab = wide[:, piece * 128:(piece + 1) * 128]
                squares = squares + slab * slab
        acc_s[here, :] = squares

    def tokens_of(side, d, h):
        j, valid = toks.at(side, d)

        def go():
            for p in range(half):
                toks.wait_pair(j, h * half + p)
            take_tokens(j // CORES, h)
        if d == 0:
            go()
        else:
            pl.when(valid)(go)

    def rows_wait(p):
        for side, distances in ((IN, [0]), (OUT, outs), (IN, ins)):
            for d in distances:
                j, valid = passes.at(side, d)
                if d == 0:
                    passes.wait_pair(j, p)
                else:
                    @pl.when(valid)
                    def _():
                        passes.wait_pair(j, p)

    def project(p, base, count, w):
        at = pl.ds(p * rows_piece, rows_piece)
        total_of = None
        for q in range(count):
            j = base + q
            part = dot(rows[j, at, :], w[pl.ds(pl.multiple_of(j * cols, cols), cols), :])
            total_of = part if total_of is None else total_of + part
        return total_of

    def rows_all(p, base, count):
        at = pl.ds(p * rows_piece, rows_piece)
        acc_mk[at, :] = project(p, base, count, wmk)
        acc_mv[at, :] = project(p, base, count, wmv)

    def prepare(c, carry):
        here = pl.ds(pl.multiple_of(c * chunk, chunk), chunk)
        scale = lax.rsqrt(jnp.sum(acc_s[here, :], axis=1, keepdims=True) / (n_tp * cols) + NORM_EPS)
        cosine, sine = cos_ref[here, :], sin_ref[here, :]

        def rotate(v):
            return v * cosine + pltpu.roll(v, KEY_DIM // 2, 1) * sine
        for h in range(heads):
            at = slice(h * KEY_DIM, (h + 1) * KEY_DIM)
            rq[here, at] = rotate(acc_q[here, at] * scale).astype(BF16)
            rk[here, at] = (rotate(acc_k[here, at] * scale) * KEY_DIM ** (-0.5)).astype(BF16)
            m = acc_m[here, at]
            mq[here, at] = (m * lax.rsqrt(jnp.mean(m * m, axis=1, keepdims=True) + NORM_EPS)).astype(BF16)
        rv[here, :] = (acc_v[here, :] * scale).astype(BF16)
        gate[here, :] = jax.nn.sigmoid(acc_g[here, :] * scale)
        return carry

    def retain(c):
        here = pl.ds(c * chunk, chunk)
        start = (c * chunk) // SEQ_LEN * SEQ_LEN
        length = (c + 1) * chunk - start
        whole = pl.ds(start, length)
        t = lax.broadcasted_iota(jnp.int32, (chunk, length), 0) + (c * chunk - start)
        s = lax.broadcasted_iota(jnp.int32, (chunk, length), 1)
        gap = (t - s).astype(F32)
        for h in range(heads):
            at = slice(h * KEY_DIM, (h + 1) * KEY_DIM)
            wide = slice(h * VALUE_DIM, (h + 1) * VALUE_DIM)
            decay = jnp.where(gap >= 0.0, jnp.exp(-rate_ref[h] * jnp.maximum(gap, 0.0)), 0.0)
            scores = dot_nt(rq[here, at], rk[whole, at]) * decay
            upper = scores.astype(BF16)
            lower = (scores - upper.astype(F32)).astype(BF16)
            value = rv[whole, wide]
            o = dot(upper, value) + dot(lower, value)
            o = o - jnp.mean(o, axis=1, keepdims=True)
            ret[here, wide] = o * lax.rsqrt(jnp.mean(o * o, axis=1, keepdims=True) + NORM_EPS)

    def assist(kv, p):
        @pl.when(is_helper)
        def _():
            at = pl.ds(p * rows_piece, rows_piece)
            base = jnp.where(so < 0, CORES, 0)
            kv_out[kv, at, :] = project(p, base, CORES * others, xw[kv]).astype(BF16)
            kv_copy(kv, p).start()

    block = total // blocks
    keys = picks * pass_rows

    def attend(n, carry):
        here = pl.ds(pl.multiple_of(n * block, block), block)
        there = pl.ds(pl.multiple_of(n * keys, keys), keys)
        for h in range(heads):
            at = slice(h * MEM_DIM, (h + 1) * MEM_DIM)
            wide = slice(h * VALUE_DIM, (h + 1) * VALUE_DIM)
            k = acc_mk[there, at]
            k = (k * lax.rsqrt(jnp.mean(k * k, axis=1, keepdims=True) + NORM_EPS)).astype(BF16)
            v = acc_mv[there, at].astype(BF16)
            exponent = jnp.exp(dot_nt(mq[here, at], k) * MEM_DIM ** (-0.5))
            mass = jnp.sum(exponent, axis=1, keepdims=True)
            o = (dot(exponent.astype(BF16), v) / mass).astype(BF16)
            lifted = dot(o, lift_ref[h])
            out_ref[here, wide] = (ret[here, wide] + gate[here, h:h + 1] * lifted).astype(BF16)
        return carry

    share = blocks // PIECES

    def attend_piece(p):
        for n in range(p * share, (p + 1) * share):
            attend(n, 0)

    def pass_waits(first, last):
        for g in range(first, last):
            for d in range(1, n_st):
                pass_wait(g, d).wait_recv()

    def load_waits():
        for i in range(2, len(pairs)):
            loads[i].wait()

    def settle(c):
        prepare(c, 0)
        retain(c)

    early_parts = min(parts, -(-picks * share // per))

    def in_tokens(p, distances):
        for d in distances:
            toks.relay(IN, d, p)

    def out_tokens(p):
        for d in outs:
            toks.relay(OUT, d, p)

    def in_rows(p, distances):
        for d in distances:
            passes.relay(IN, d, p)

    def out_rows(p):
        for d in outs:
            passes.relay(OUT, d, p)

    near, far = ins[:1], ins[1:]

    @pl.when(is_edge)
    def _():
        in_tokens(0, near)
        in_tokens(1, near)
        pass_waits(0, early_parts)
        build_piece(0)
        passes.send_own(0)
        passes.share_own(0)
        for p in range(half, PIECES):
            toks.send_own(p)
        lend_all(late, lent)
        in_tokens(2, near)
        load_waits()
        tokens_of(IN, 0, 0)
        in_tokens(3, near)
        pass_waits(early_parts, parts)
        for p in range(1, PIECES):
            build_piece(p)
            passes.send_own(p)
            passes.share_own(p)
        tokens_of(IN, 0, 1)
        in_tokens(0, ins[1:2])
        tokens_of(IN, 1, 0)
        in_tokens(1, ins[1:2])
        tokens_of(IN, 1, 1)
        in_tokens(2, ins[1:2])
        tokens_of(IN, 2, 0)
        in_tokens(3, ins[1:2])
        tokens_of(IN, 2, 1)
        for p in range(PIECES):
            passes.wait_pair(me, p)
            rows_all(p, z * CORES, CORES)
        for d in ins[2:]:
            in_tokens(0, [d])
            in_tokens(1, [d])
            tokens_of(IN, d, 0)
        settle(0)
        settle(1)
        for d in ins[2:]:
            in_tokens(2, [d])
            in_tokens(3, [d])
            tokens_of(IN, d, 1)
        settle(2)
        settle(3)
        for p in range(PIECES):
            at = pl.ds(p * rows_piece, rows_piece)
            for kv, acc in ((0, acc_mk), (1, acc_mv)):
                kv_copy(kv, p).wait_recv()
                acc[at, :] += kv_in[kv, at, :].astype(F32)
            attend_piece(p)
        for w in range(lent):
            for part in range(2):
                lend(w, part).wait_send()

    @pl.when(depth > 0)
    def _():
        in_tokens(0, near)
        spread_own(0, 1)
        in_tokens(1, near)
        out_tokens(0)
        in_tokens(2, near)
        spread_own(1, 2)
        pass_waits(0, early_parts)
        build_piece(0)
        passes.send_own(0)
        passes.share_own(0)
        in_tokens(3, near)
        out_tokens(1)
        load_waits()
        tokens_of(IN, 0, 0)
        in_tokens(0, far)
        spread_own(2, 3)
        pass_waits(early_parts, parts)
        for p in range(1, PIECES):
            build_piece(p)
            passes.send_own(p)
            passes.share_own(p)
        tokens_of(IN, 0, 1)
        in_rows(0, near)
        spread_own(3, late)
        tokens_of(IN, 1, 0)
        in_tokens(1, far)
        out_rows(0)
        tokens_of(IN, 1, 1)
        for d in outs:
            tokens_of(OUT, d, 0)
        out_tokens(2)
        in_rows(1, near)
        spread_on(0, others - 1)
        for d in far:
            tokens_of(IN, d, 0)
        out_tokens(3)
        in_rows(2, near)
        spread_on(others - 1, others)
        settle(0)
        settle(1)
        in_rows(3, near)
        spread_own(late, late + 1)
        in_rows(0, far)
        rows_wait(0)
        spread_own(late + 1, lent)
        spread_last(0)
        assist(0, 0)
        spread_on(others, late)
        for d in outs:
            tokens_of(OUT, d, 1)
        in_tokens(2, far)
        out_rows(1)
        spread_on(late, late + 1)
        in_tokens(3, far)
        out_rows(2)
        spread_on(late + 1, lent)
        for d in far:
            tokens_of(IN, d, 1)
        out_rows(3)
        in_rows(1, far)
        rows_wait(1)
        assist(0, 1)
        spread_last(1)
        assist(1, 0)
        assist(1, 1)
        settle(2)
        settle(3)
        in_rows(2, far)
        rows_wait(2)
        assist(0, 2)
        assist(1, 2)
        rows_all(0, 0, n_tp)
        attend_piece(0)
        in_rows(3, far)
        rows_wait(3)
        assist(0, 3)
        assist(1, 3)
        for p in range(1, PIECES):
            rows_all(p, 0, n_tp)
            attend_piece(p)

        @pl.when(is_helper)
        def _():
            spread_drain()
            for kv in range(2):
                for p in range(PIECES):
                    kv_copy(kv, p).wait_send()

    for d in range(1, n_st):
        id_copy(d).wait_send()
        for g in range(parts):
            pass_copy(g, d).wait_send()
    toks.drain()
    passes.drain()


def rotary_tables(total):
    half = KEY_DIM // 2
    angle = (np.arange(total) % SEQ_LEN)[:, None] * ROPE_BASE ** (-np.arange(half) / half)[None, :]
    cosine, sine = np.cos(angle), np.sin(angle)
    return (np.concatenate([cosine, cosine], 1).astype(np.float32),
            np.concatenate([-sine, sine], 1).astype(np.float32))


def solution(mesh):
    n_st, n_tp = mesh.shape["st"], mesh.shape["tp"]
    n_z = n_tp // CORES
    assert n_z >= 4

    def per_device(tokens, w_query, w_key, w_value, w_mem_query, w_mem_key, w_mem_value, w_gate, w_lift,
                   decay_rate, store, passage_ids):
        total, cols = tokens.shape
        heads = decay_rate.shape[0]
        blocks, picks = passage_ids.shape
        requests = blocks * picks
        held, pass_rows, _ = store.shape
        cap = max(1, 2 * requests // n_st)
        parts = cap // picks if cap % picks == 0 else 1
        cosine, sine = rotary_tables(total)
        hbm = pl.BlockSpec(memory_space=pl.ANY)
        vmem = pl.BlockSpec(memory_space=pltpu.VMEM)
        smem = pl.BlockSpec(memory_space=pltpu.SMEM)
        V = pltpu.VMEM
        dma = pltpu.SemaphoreType.DMA
        wide = w_value.shape[1]
        key_cols, mem_cols = w_query.shape[1], w_mem_query.shape[1]
        n_b = square_split(n_st)
        n_mates = n_b - 1 + n_st // n_b - 1

        def flow_sems():
            return dma((n_tp, PIECES)), dma((n_tp, PIECES)), dma((PIECES,)), dma((n_tp, PIECES))
        all_rows = requests * pass_rows
        scratch = [
            V((n_tp, total, cols), BF16), V((n_tp, all_rows, cols), BF16),
            V(cosine.shape, F32), V(sine.shape, F32), V(w_lift.shape, BF16),
            V(w_query.shape, BF16), V(w_key.shape, BF16), V(w_value.shape, BF16),
            V(w_mem_query.shape, BF16), V(w_mem_key.shape, BF16), V(w_mem_value.shape, BF16),
            V(store.shape, BF16), V((n_st, cap, pass_rows, cols), BF16),
            tuple(V((n_st, cap // parts, pass_rows, cols), BF16) for _ in range(parts)),
            V((n_st, picks, blocks), jnp.int32), pltpu.SMEM((n_st, picks, blocks), jnp.int32),
            V((total, key_cols), F32), V((total, key_cols), F32), V((total, wide), F32), V((total, mem_cols), F32),
            V((total, heads), F32), V((total, 128), F32),
            V((all_rows, mem_cols), F32), V((all_rows, mem_cols), F32),
            V((total, key_cols), BF16), V((total, key_cols), BF16), V((total, wide), BF16), V((total, mem_cols), BF16),
            V((total, wide), F32), V((total, heads), F32),
            V(w_mem_key.shape, BF16), V(w_mem_value.shape, BF16),
            V((2, all_rows, mem_cols), BF16), V((2, all_rows, mem_cols), BF16),
            dma((16,)), dma((n_st,)), dma((n_st,)), dma((parts, n_st)), dma((parts, n_st)),
            flow_sems(), flow_sems(),
            dma((2, n_z - 1, 2)), dma((2, n_z - 1, 2, n_st)), dma((2, n_mates, n_st)), dma((2, PIECES)), dma((2, PIECES)),
        ]
        return pl.pallas_call(
            functools.partial(kernel, n_st, n_tp, cap, picks, held),
            out_shape=jax.ShapeDtypeStruct((total, heads * VALUE_DIM), BF16),
            in_specs=[smem] + [hbm] * 7 + [vmem] + [hbm] * 5,
            out_specs=vmem,
            scratch_shapes=scratch,
            compiler_params=pltpu.CompilerParams(
                collective_id=0, has_side_effects=True, vmem_limit_bytes=60 * 1024 * 1024),
        )(decay_rate, tokens, w_query, w_key, w_value, w_mem_query, w_mem_key, w_mem_value,
          w_gate.T, w_lift, jnp.asarray(cosine), jnp.asarray(sine), store, passage_ids.T)

    in_specs = (P("st", "tp"),) + (P(None, "tp"),) * 7 + (
        P("tp", None, None), P("tp"), P("st", None, "tp"), P("st", None))
    return jax.shard_map(per_device, mesh=mesh, in_specs=in_specs, out_specs=P("st", "tp"), check_vma=False)
```

```python
import functools

import jax
import jax.numpy as jnp
import numpy as np
from jax import lax
from jax.experimental import pallas as pl
from jax.experimental.pallas import tpu as pltpu
from jax.sharding import PartitionSpec as P

KEY_DIM = 128
VALUE_DIM = 256
MEM_DIM = 128
SEQ_LEN = 512
NORM_EPS = 1e-06
ROPE_BASE = 10000.0
CORES = 2
PIECES = 4
OUT, IN = 0, 1
MESH = pl.DeviceIdType.MESH
F32 = jnp.float32
BF16 = jnp.bfloat16


def dot(a, b):
    return jnp.dot(a, b, preferred_element_type=F32)


def dot_nt(a, b):
    return lax.dot_general(a, b, (((1,), (1,)), ((), ())), preferred_element_type=F32)


def square_split(n):
    return 1 << ((n.bit_length() - 1) // 2)


def kernel(
    n_st, n_tp, cap, picks, held,
    rate_ref, tok_hbm, wq_hbm, wk_hbm, wv_hbm, wm_hbm, wmk_hbm, wmv_hbm, wg_ref, lift_hbm,
    cos_hbm, sin_hbm, store_hbm, ids_hbm,
    out_ref,
    tok, rows, cos_ref, sin_ref, lift_ref, wq, wk, wv, wm, wmk, wmv, store, slots, landed, ids_v, ids_s,
    acc_q, acc_k, acc_v, acc_m, acc_g, acc_s, acc_mk, acc_mv,
    rq, rk, rv, mq, ret, gate, xwk, xwv, kv_out, kv_in,
    load_sem, id_send, id_recv, pass_send, pass_recv,
    t_sems, r_sems, w_send, w_own, w_row, w_col, w_final, spread_send, kv_send, kv_recv,
):
    st = lax.axis_index("st")
    me = lax.axis_index("tp")
    z = me // CORES
    core = me % CORES
    n_z = n_tp // CORES
    total, cols = tok.shape[1:]
    heads = mq.shape[1] // MEM_DIM
    mem_cols = mq.shape[1]
    requests = ids_s.shape[1] * ids_s.shape[2]
    blocks = requests // picks
    pass_rows = store.shape[1]
    parts = len(landed)
    per = cap // parts
    chunk = total // PIECES
    rows_piece = rows.shape[1] // PIECES
    half = PIECES // 2

    so = jnp.where(z < n_z // 2, -1, 1)
    depth = jnp.minimum(z, n_z - 1 - z)
    edge_z = z + so * depth
    is_edge = depth == 0
    is_helper = depth == 1
    me_out = me + CORES * so
    me_in = me - CORES * so
    pair = me + 1 - 2 * core
    outs = range(1, (n_z - 1) // 2 + 1)
    ins = range(1, n_z)

    loads = []
    pairs = [(store_hbm, store), (ids_hbm, ids_v.at[st]), (tok_hbm, tok.at[me]), (wq_hbm, wq), (wk_hbm, wk),
             (wv_hbm, wv), (wm_hbm, wm), (wmk_hbm, wmk), (wmv_hbm, wmv),
             (cos_hbm, cos_ref), (sin_hbm, sin_ref), (lift_hbm, lift_ref)]
    for i, (src, dst) in enumerate(pairs):
        loads.append(pltpu.make_async_copy(src, dst, load_sem.at[i]))
    loads[1].start()
    loads[0].start()

    barrier = pltpu.get_barrier_semaphore()

    def greet(to_st, to_tp):
        pl.semaphore_signal(barrier, inc=1, device_id=(to_st, to_tp), device_id_type=MESH)

    @pl.when(depth > 0)
    def _():
        greet(st, me_out)
    greet(st, me_in)
    greet(st, pair)
    for d in range(1, n_st):
        greet((st + d) % n_st, me)
    pl.semaphore_wait(barrier, n_st + 1 + (depth > 0).astype(jnp.int32))

    def remote(src, dst, send, recv, to_st, to_tp):
        return pltpu.make_async_remote_copy(
            src_ref=src, dst_ref=dst, send_sem=send, recv_sem=recv,
            device_id=(to_st, to_tp), device_id_type=MESH)

    class Flow:
        def __init__(self, buf, sems, floor, pair_sem, source=None):
            self.buf, self.floor, self.source, self.pair_sem = buf, floor, source, pair_sem
            self.recv, self.recv_pair, self.send, self.own_out, self.send_pair = sems
            self.size = buf.shape[1] // PIECES

        def piece(self, j, p):
            return self.buf.at[j, pl.ds(p * self.size, self.size)]

        def origin(self, p):
            return self.piece(me, p) if self.source is None else self.source.at[pl.ds(p * self.size, self.size)]

        def along_z(self, j, p, to, src=None, send=None):
            return remote(self.piece(j, p) if src is None else src, self.piece(j, p),
                          self.send.at[j // CORES] if send is None else send, self.recv.at[j // CORES, p], st, to)

        def to_pair(self, j, p, src=None):
            return remote(self.piece(j, p) if src is None else src, self.piece(j, p),
                          self.send_pair.at[0], self.pair_sem(self.recv_pair, j // CORES, p), st, pair)

        def send_own(self, p):
            self.along_z(me, p, me_in, self.origin(p)).start()

            @pl.when(depth > self.floor)
            def _():
                self.along_z(me, p, me_out, self.origin(p), self.own_out.at[0]).start()

        def share_own(self, p):
            self.to_pair(me, p, self.origin(p)).start()

        def at(self, side, d):
            far = CORES * so * d
            if side == OUT:
                return me + far, d <= depth
            return me - far, (d <= n_z - 1 - depth) & (depth >= self.floor)

        def relay(self, side, d, p):
            j, valid = self.at(side, d)

            @pl.when(valid)
            def _():
                self.along_z(j, p, me_in).wait_recv()
                if side == OUT:
                    self.along_z(j, p, me_in).start()
                else:
                    @pl.when(depth > self.floor)
                    def _():
                        self.along_z(j, p, me_out).start()
                self.to_pair(j, p).start()

        def wait_pair(self, ref, sem):
            remote(ref, ref, self.send_pair.at[0], sem, st, pair).wait_recv()

        def drain(self):
            def sent(ref, sem):
                remote(ref, ref, sem, self.recv.at[0, 0], st, me_in).wait_send()
            sent(self.buf.at[0], self.send.at[z])

            @pl.when(depth > self.floor)
            def _():
                sent(self.buf.at[0], self.own_out.at[0])
            for side, distances in ((OUT, outs), (IN, ins)):
                for d in distances:
                    j, valid = self.at(side, d)

                    @pl.when(valid if side == OUT else valid & (depth > self.floor))
                    def _():
                        sent(self.buf.at[0], self.send.at[j // CORES])

            @pl.when(depth >= self.floor)
            def _():
                sent(self.buf.at[pl.ds(0, n_z)], self.send_pair.at[0])

            @pl.when(depth < self.floor)
            def _():
                sent(self.buf.at[0], self.send_pair.at[0])

    toks = Flow(tok, t_sems, 0, lambda sems, chip, p: sems.at[chip, p // half], tok_hbm)
    passes = Flow(rows, r_sems, 1, lambda sems, chip, p: sems.at[p])

    n_b = square_split(n_st)
    n_a = n_st // n_b
    a, b = st // n_b, st % n_b
    row_mates = [a * n_b + (b + i) % n_b for i in range(1, n_b)]
    col_mates = [(a + i) % n_a * n_b + b for i in range(1, n_a)]
    mates = row_mates + col_mates
    along_row = range(0, n_b - 1)
    along_col = range(n_b - 1, len(mates))
    sub = CORES * cols // n_st // 2
    others = n_z - 1
    lent = 2 * others
    late = lent - 2
    xw = (xwk, xwv)

    def lent_at(e, part, s, count=1):
        start = (edge_z - so * (e + 1)) * (CORES * cols) + (2 * s + part) * sub
        return pl.ds(pl.multiple_of(start, sub), sub * count)

    def lend(w):
        kv, e = w // others, w % others
        at = lent_at(e, 0, st, 2)
        return remote((wmk_hbm, wmv_hbm)[kv].at[at], xw[kv].at[at], w_send.at[0], w_own.at[w], st, me_in)

    def lend_all(first, last):
        for w in range(first, last):
            lend(w).start()

    def spread(w, part, s, i, send, recv):
        kv, e = w // others, w % others
        here = xw[kv].at[lent_at(e, part, s)]
        return remote(here, here, spread_send.at[send], recv, mates[i], me)

    def spread_own(first, last):
        @pl.when(is_helper)
        def _():
            for w in range(first, last):
                lend(w).wait_recv()
                for part in range(2):
                    for i in along_row:
                        recv = w_row.at[w, n_b - 2 - i] if part == 0 else w_final.at[w // others]
                        spread(w, part, st, i, 0, recv).start()
                    for i in along_col:
                        recv = w_col.at[w, n_a - 2 - (i - (n_b - 1))] if part == 1 else w_final.at[w // others]
                        spread(w, part, st, i, 0, recv).start()

    def spread_on(first, last):
        @pl.when(is_helper)
        def _():
            for w in range(first, last):
                final = w_final.at[w // others]
                for k, s in enumerate(row_mates):
                    spread(w, 0, s, 0, 1, w_row.at[w, k]).wait_recv()
                    for i in along_col:
                        spread(w, 0, s, i, 1, final).start()
                for k, s in enumerate(col_mates):
                    spread(w, 1, s, 0, 1, w_col.at[w, k]).wait_recv()
                    for i in along_row:
                        spread(w, 1, s, i, 1, final).start()

    def lent_rows(count):
        return xwk.at[pl.ds(0, count * sub)]

    def spread_last(kv):
        @pl.when(is_helper)
        def _():
            whole = lent_rows(others * (n_b * (n_a - 1) + n_a * (n_b - 1)))
            remote(whole, whole, spread_send.at[0], w_final.at[kv], st, me_in).wait_recv()

    def spread_drain():
        for k, count in enumerate((2 * len(mates), 2 * (n_a - 1) * (n_b - 1))):
            whole = lent_rows(2 * others * count)
            remote(whole, whole, spread_send.at[k], w_final.at[0], st, me_in).wait_send()

    def lend_drain():
        whole = lent_rows(2 * others * 2)
        remote(whole, whole, w_send.at[0], w_own.at[0], st, me_in).wait_send()

    def kv_copy(kv, p):
        at = pl.ds(pl.multiple_of(p * rows_piece, rows_piece), rows_piece)
        return remote(kv_out.at[kv, at], kv_in.at[kv, at], kv_send.at[0], kv_recv.at[kv, p], st, me_out)

    def id_copy(d):
        return remote(ids_v.at[st], ids_v.at[st], id_send.at[d], id_recv.at[st], (st + d) % n_st, me)

    def id_wait(d):
        other = (st + d) % n_st
        return remote(ids_v.at[other], ids_v.at[other], id_send.at[d], id_recv.at[other], other, me)

    loads[1].wait()
    for d in range(1, n_st):
        id_copy(d).start()

    @pl.when(is_edge)
    def _():
        for p in range(half):
            lend_all(p, p + 1)
            toks.send_own(p)
        lend_all(half, late)

    @pl.when(depth > 0)
    def _():
        for p in range(PIECES):
            toks.send_own(p)
    for p in range(PIECES):
        toks.share_own(p)
    loads[2].start()

    for ref in (acc_q, acc_k, acc_v, acc_m, acc_g, acc_s):
        ref[...] = jnp.zeros_like(ref)

    for d in range(1, n_st):
        id_wait(d).wait_recv()
    to_scalar = pltpu.make_async_copy(ids_v, ids_s, load_sem.at[len(pairs)])
    to_scalar.start()
    to_scalar.wait()
    loads[0].wait()
    for i in range(3, len(pairs)):
        loads[i].start()

    def asked(source, k):
        found = jnp.int32(0)
        seen = jnp.int32(0)
        for i in range(requests):
            ident = ids_s[source, i % picks, i // picks]
            mine = (ident // held) == st
            found = jnp.where(mine & (seen == k), ident % held, found)
            seen = seen + mine.astype(jnp.int32)
        return found

    def pass_copy(g, d):
        return remote(slots.at[d, pl.ds(g * per, per)], landed[g].at[st], pass_send.at[0], pass_recv.at[g],
                      (st + d) % n_st, me)

    def pass_waits(first, last):
        for g in range(first, last):
            all_of = landed[g].at[pl.ds(0, n_st - 1)]
            remote(all_of, all_of, pass_send.at[0], pass_recv.at[g], (st + 1) % n_st, me).wait_recv()

    for g in range(parts):
        def fill(d, carry):
            for k in range(g * per, (g + 1) * per):
                slots[d, k] = store[asked((st + d) % n_st, k)]
            return carry
        lax.fori_loop(1, n_st, fill, 0)
        for d in range(1, n_st):
            pass_copy(g, d).start()
    for k in range(cap):
        landed[k // per][st, k % per] = store[asked(st, k)]

    def build(block):
        reach = min(parts, -(-picks * (block + 1) // per))
        for i in range(block * picks, (block + 1) * picks):
            ident = ids_s[st, i % picks, i // picks]
            owner = ident // held
            order = jnp.int32(0)
            for e in range(i):
                order = order + ((ids_s[st, e % picks, e // picks] // held) == owner).astype(jnp.int32)
            value = landed[0][owner, jnp.minimum(order, per - 1)]
            for g in range(1, reach):
                other = landed[g][owner, jnp.clip(order - g * per, 0, per - 1)]
                value = jnp.where(order >= g * per, other, value)
            rows[me, pl.ds(i * pass_rows, pass_rows), :] = value

    def build_piece(p):
        for block in range(p * blocks // PIECES, (p + 1) * blocks // PIECES):
            build(block)

    def take_tokens(at_z, h):
        here = pl.ds(pl.multiple_of(h * (half * chunk), half * chunk), half * chunk)
        xs, ats = [], []
        for c in range(CORES):
            j = at_z * CORES + c
            xs.append(tok[j, here, :])
            ats.append(pl.ds(pl.multiple_of(j * cols, cols), cols))
        for acc, w in ((acc_q, wq), (acc_k, wk), (acc_v, wv), (acc_m, wm)):
            acc[here, :] += sum(dot(x, w[at, :]) for x, at in zip(xs, ats))
        squares = acc_s[here, :]
        for x, at in zip(xs, ats):
            wide = x.astype(F32)
            if heads > 1:
                acc_g[here, :] += dot_nt(x, wg_ref[:, at])
            else:
                acc_g[here, :] += jnp.sum(wide * wg_ref[:, at].astype(F32), axis=1, keepdims=True)
            for piece in range(cols // 128):
                slab = wide[:, piece * 128:(piece + 1) * 128]
                squares = squares + slab * slab
        acc_s[here, :] = squares

    def tokens_of(side, d, h):
        j, valid = toks.at(side, d)

        def go():
            toks.wait_pair(tok.at[j + 1 - 2 * core, pl.ds(h * half * chunk, half * chunk)],
                           toks.recv_pair.at[j // CORES, h])
            take_tokens(j // CORES, h)
        if d == 0:
            go()
        else:
            pl.when(valid)(go)

    def rows_wait(p, chips):
        passes.wait_pair(rows.at[pl.ds(0, chips), pl.ds(p * rows_piece, rows_piece)], passes.recv_pair.at[p])

    def project(p, base, count, w):
        at = pl.ds(p * rows_piece, rows_piece)
        total_of = None
        for q in range(count):
            j = base + q
            part = dot(rows[j, at, :], w[pl.ds(pl.multiple_of(j * cols, cols), cols), :])
            total_of = part if total_of is None else total_of + part
        return total_of

    def rows_all(p, base, count):
        at = pl.ds(p * rows_piece, rows_piece)
        acc_mk[at, :] = project(p, base, count, wmk)
        acc_mv[at, :] = project(p, base, count, wmv)

    def prepare(c, carry):
        here = pl.ds(pl.multiple_of(c * chunk, chunk), chunk)
        scale = lax.rsqrt(jnp.sum(acc_s[here, :], axis=1, keepdims=True) / (n_tp * cols) + NORM_EPS)
        cosine, sine = cos_ref[here, :], sin_ref[here, :]

        def rotate(v):
            return v * cosine + pltpu.roll(v, KEY_DIM // 2, 1) * sine
        for h in range(heads):
            at = slice(h * KEY_DIM, (h + 1) * KEY_DIM)
            rq[here, at] = rotate(acc_q[here, at] * scale).astype(BF16)
            rk[here, at] = (rotate(acc_k[here, at] * scale) * KEY_DIM ** (-0.5)).astype(BF16)
            m = acc_m[here, at]
            mq[here, at] = (m * lax.rsqrt(jnp.mean(m * m, axis=1, keepdims=True) + NORM_EPS)).astype(BF16)
        rv[here, :] = (acc_v[here, :] * scale).astype(BF16)
        gate[here, :] = jax.nn.sigmoid(acc_g[here, :] * scale)
        return carry

    def retain(c):
        here = pl.ds(c * chunk, chunk)
        start = (c * chunk) // SEQ_LEN * SEQ_LEN
        length = (c + 1) * chunk - start
        whole = pl.ds(start, length)
        t = lax.broadcasted_iota(jnp.int32, (chunk, length), 0) + (c * chunk - start)
        s = lax.broadcasted_iota(jnp.int32, (chunk, length), 1)
        gap = (t - s).astype(F32)
        for h in range(heads):
            at = slice(h * KEY_DIM, (h + 1) * KEY_DIM)
            wide = slice(h * VALUE_DIM, (h + 1) * VALUE_DIM)
            decay = jnp.where(gap >= 0.0, jnp.exp(-rate_ref[h] * jnp.maximum(gap, 0.0)), 0.0)
            scores = dot_nt(rq[here, at], rk[whole, at]) * decay
            upper = scores.astype(BF16)
            lower = (scores - upper.astype(F32)).astype(BF16)
            value = rv[whole, wide]
            o = dot(upper, value) + dot(lower, value)
            o = o - jnp.mean(o, axis=1, keepdims=True)
            ret[here, wide] = o * lax.rsqrt(jnp.mean(o * o, axis=1, keepdims=True) + NORM_EPS)

    def assist(kv, p):
        @pl.when(is_helper)
        def _():
            at = pl.ds(p * rows_piece, rows_piece)
            base = jnp.where(so < 0, CORES, 0)
            kv_out[kv, at, :] = project(p, base, CORES * others, xw[kv]).astype(BF16)
            kv_copy(kv, p).start()

    block = total // blocks
    keys = picks * pass_rows

    def attend(n, carry):
        here = pl.ds(pl.multiple_of(n * block, block), block)
        there = pl.ds(pl.multiple_of(n * keys, keys), keys)
        for h in range(heads):
            at = slice(h * MEM_DIM, (h + 1) * MEM_DIM)
            wide = slice(h * VALUE_DIM, (h + 1) * VALUE_DIM)
            k = acc_mk[there, at]
            k = (k * lax.rsqrt(jnp.mean(k * k, axis=1, keepdims=True) + NORM_EPS)).astype(BF16)
            v = acc_mv[there, at].astype(BF16)
            exponent = jnp.exp(dot_nt(mq[here, at], k) * MEM_DIM ** (-0.5))
            mass = jnp.sum(exponent, axis=1, keepdims=True)
            o = (dot(exponent.astype(BF16), v) / mass).astype(BF16)
            lifted = dot(o, lift_ref[h])
            out_ref[here, wide] = (ret[here, wide] + gate[here, h:h + 1] * lifted).astype(BF16)
        return carry

    share = blocks // PIECES

    def attend_piece(p):
        for n in range(p * share, (p + 1) * share):
            attend(n, 0)

    def load_waits():
        for i in range(2, len(pairs)):
            loads[i].wait()

    def settle(c):
        prepare(c, 0)
        retain(c)

    early_parts = min(parts, -(-picks * share // per))

    def in_tokens(p, distances):
        for d in distances:
            toks.relay(IN, d, p)

    def out_tokens(p):
        for d in outs:
            toks.relay(OUT, d, p)

    def in_rows(p, distances):
        for d in distances:
            passes.relay(IN, d, p)

    def out_rows(p):
        for d in outs:
            passes.relay(OUT, d, p)

    near, far = ins[:1], ins[1:]

    @pl.when(is_edge)
    def _():
        in_tokens(0, near)
        in_tokens(1, near)
        pass_waits(0, early_parts)
        build_piece(0)
        passes.send_own(0)
        passes.share_own(0)
        for p in range(half, PIECES):
            toks.send_own(p)
        lend_all(late, lent)
        in_tokens(2, near)
        load_waits()
        tokens_of(IN, 0, 0)
        in_tokens(3, near)
        pass_waits(early_parts, parts)
        for p in range(1, PIECES):
            build_piece(p)
            passes.send_own(p)
            passes.share_own(p)
        tokens_of(IN, 0, 1)
        in_tokens(0, ins[1:2])
        tokens_of(IN, 1, 0)
        in_tokens(1, ins[1:2])
        tokens_of(IN, 1, 1)
        in_tokens(2, ins[1:2])
        tokens_of(IN, 2, 0)
        in_tokens(3, ins[1:2])
        tokens_of(IN, 2, 1)
        for p in range(PIECES):
            rows_wait(p, 1)
            rows_all(p, z * CORES, CORES)
        for d in ins[2:]:
            in_tokens(0, [d])
            in_tokens(1, [d])
            tokens_of(IN, d, 0)
        settle(0)
        settle(1)
        for d in ins[2:]:
            in_tokens(2, [d])
            in_tokens(3, [d])
            tokens_of(IN, d, 1)
        settle(2)
        settle(3)
        for p in range(PIECES):
            at = pl.ds(p * rows_piece, rows_piece)
            for kv, acc in ((0, acc_mk), (1, acc_mv)):
                kv_copy(kv, p).wait_recv()
                acc[at, :] += kv_in[kv, at, :].astype(F32)
            attend_piece(p)
        lend_drain()

    @pl.when(depth > 0)
    def _():
        in_tokens(0, near)
        spread_own(0, 1)
        in_tokens(1, near)
        out_tokens(0)
        in_tokens(2, near)
        spread_own(1, 2)
        pass_waits(0, early_parts)
        build_piece(0)
        passes.send_own(0)
        passes.share_own(0)
        in_tokens(3, near)
        out_tokens(1)
        load_waits()
        tokens_of(IN, 0, 0)
        in_tokens(0, far)
        spread_own(2, 3)
        pass_waits(early_parts, parts)
        for p in range(1, PIECES):
            build_piece(p)
            if p < PIECES - 1:
                passes.send_own(p)
            passes.share_own(p)
        tokens_of(IN, 0, 1)
        in_rows(0, near)
        spread_own(3, late)
        tokens_of(IN, 1, 0)
        in_tokens(1, far)
        out_rows(0)
        tokens_of(IN, 1, 1)
        for d in outs:
            tokens_of(OUT, d, 0)
        out_tokens(2)
        in_rows(1, near)
        spread_on(0, others - 1)
        for d in far:
            tokens_of(IN, d, 0)
        out_tokens(3)
        passes.send_own(PIECES - 1)
        in_rows(2, near)
        spread_on(others - 1, others)
        in_tokens(2, far)
        spread_own(late, late + 1)
        settle(0)
        settle(1)
        in_tokens(3, far)
        spread_own(late + 1, lent)
        spread_on(others, late)
        for d in outs:
            tokens_of(OUT, d, 1)
        in_rows(3, near)
        in_rows(0, far)
        rows_wait(0, n_z)
        spread_last(0)
        assist(0, 0)
        out_rows(1)
        spread_on(late, late + 1)
        for d in far:
            tokens_of(IN, d, 1)
        out_rows(2)
        spread_on(late + 1, lent)
        out_rows(3)
        in_rows(1, far)
        rows_wait(1, n_z)
        assist(0, 1)
        spread_last(1)
        assist(1, 0)
        assist(1, 1)
        in_rows(2, far)
        settle(2)
        rows_wait(2, n_z)
        assist(0, 2)
        assist(1, 2)
        settle(3)
        in_rows(3, far)
        rows_all(0, 0, n_tp)
        rows_wait(3, n_z)
        assist(0, 3)
        assist(1, 3)
        attend_piece(0)
        for p in range(1, PIECES):
            rows_all(p, 0, n_tp)
            attend_piece(p)

        @pl.when(is_helper)
        def _():
            spread_drain()
            remote(kv_out, kv_in, kv_send.at[0], kv_recv.at[0, 0], st, me_out).wait_send()

    for d in range(1, n_st):
        id_copy(d).wait_send()
    all_slots = slots.at[pl.ds(1, n_st - 1)]
    remote(all_slots, all_slots, pass_send.at[0], pass_recv.at[0], (st + 1) % n_st, me).wait_send()
    toks.drain()
    passes.drain()


def rotary_tables(total):
    half = KEY_DIM // 2
    angle = (np.arange(total) % SEQ_LEN)[:, None] * ROPE_BASE ** (-np.arange(half) / half)[None, :]
    cosine, sine = np.cos(angle), np.sin(angle)
    return (np.concatenate([cosine, cosine], 1).astype(np.float32),
            np.concatenate([-sine, sine], 1).astype(np.float32))


def solution(mesh):
    n_st, n_tp = mesh.shape["st"], mesh.shape["tp"]
    n_z = n_tp // CORES
    assert n_z >= 4

    def per_device(tokens, w_query, w_key, w_value, w_mem_query, w_mem_key, w_mem_value, w_gate, w_lift,
                   decay_rate, store, passage_ids):
        total, cols = tokens.shape
        heads = decay_rate.shape[0]
        blocks, picks = passage_ids.shape
        requests = blocks * picks
        held, pass_rows, _ = store.shape
        cap = max(1, 2 * requests // n_st)
        parts = cap // picks if cap % picks == 0 else 1
        cosine, sine = rotary_tables(total)
        hbm = pl.BlockSpec(memory_space=pl.ANY)
        vmem = pl.BlockSpec(memory_space=pltpu.VMEM)
        smem = pl.BlockSpec(memory_space=pltpu.SMEM)
        V = pltpu.VMEM
        dma = pltpu.SemaphoreType.DMA
        wide = w_value.shape[1]
        key_cols, mem_cols = w_query.shape[1], w_mem_query.shape[1]
        n_b = square_split(n_st)

        def flow_sems(*pair_shape):
            return dma((n_z, PIECES)), dma(pair_shape), dma((n_z,)), dma((1,)), dma((1,))
        all_rows = requests * pass_rows
        scratch = [
            V((n_tp, total, cols), BF16), V((n_tp, all_rows, cols), BF16),
            V(cosine.shape, F32), V(sine.shape, F32), V(w_lift.shape, BF16),
            V(w_query.shape, BF16), V(w_key.shape, BF16), V(w_value.shape, BF16),
            V(w_mem_query.shape, BF16), V(w_mem_key.shape, BF16), V(w_mem_value.shape, BF16),
            V(store.shape, BF16), V((n_st, cap, pass_rows, cols), BF16),
            tuple(V((n_st, cap // parts, pass_rows, cols), BF16) for _ in range(parts)),
            V((n_st, picks, blocks), jnp.int32), pltpu.SMEM((n_st, picks, blocks), jnp.int32),
            V((total, key_cols), F32), V((total, key_cols), F32), V((total, wide), F32), V((total, mem_cols), F32),
            V((total, heads), F32), V((total, 128), F32),
            V((all_rows, mem_cols), F32), V((all_rows, mem_cols), F32),
            V((total, key_cols), BF16), V((total, key_cols), BF16), V((total, wide), BF16), V((total, mem_cols), BF16),
            V((total, wide), F32), V((total, heads), F32),
            V(w_mem_key.shape, BF16), V(w_mem_value.shape, BF16),
            V((2, all_rows, mem_cols), BF16), V((2, all_rows, mem_cols), BF16),
            dma((13,)), dma((n_st,)), dma((n_st,)), dma((1,)), dma((parts,)),
            flow_sems(n_z, 2), flow_sems(PIECES),
            dma((1,)), dma((2 * (n_z - 1),)), dma((2 * (n_z - 1), n_b - 1)), dma((2 * (n_z - 1), n_st // n_b - 1)),
            dma((2,)), dma((2,)), dma((1,)), dma((2, PIECES)),
        ]
        return pl.pallas_call(
            functools.partial(kernel, n_st, n_tp, cap, picks, held),
            out_shape=pltpu.VMEM((total, heads * VALUE_DIM), BF16),
            in_specs=[smem] + [hbm] * 7 + [vmem] + [hbm] * 5,
            out_specs=vmem,
            scratch_shapes=scratch,
            compiler_params=pltpu.CompilerParams(
                collective_id=0, has_side_effects=True, vmem_limit_bytes=60 * 1024 * 1024),
        )(decay_rate, tokens, w_query, w_key, w_value, w_mem_query, w_mem_key, w_mem_value,
          w_gate.T, w_lift, jnp.asarray(cosine), jnp.asarray(sine), store, passage_ids.T)

    in_specs = (P("st", "tp"),) + (P(None, "tp"),) * 7 + (
        P("tp", None, None), P("tp"), P("st", None, "tp"), P("st", None))
    return jax.shard_map(per_device, mesh=mesh, in_specs=in_specs, out_specs=P("st", "tp"), check_vma=False)
```

```python
import functools

import jax
import jax.numpy as jnp
import numpy as np
from jax import lax
from jax.experimental import pallas as pl
from jax.experimental.pallas import tpu as pltpu
from jax.sharding import PartitionSpec as P

KEY_DIM = 128
VALUE_DIM = 256
MEM_DIM = 128
SEQ_LEN = 512
NORM_EPS = 1e-06
ROPE_BASE = 10000.0
CORES = 2
PIECES = 4
OUT, IN = 0, 1
MESH = pl.DeviceIdType.MESH
F32 = jnp.float32
BF16 = jnp.bfloat16


def dot(a, b):
    return jnp.dot(a, b, preferred_element_type=F32)


def dot_nt(a, b):
    return lax.dot_general(a, b, (((1,), (1,)), ((), ())), preferred_element_type=F32)


def square_split(n):
    return 1 << ((n.bit_length() - 1) // 2)


def row_bounds(blocks, keys):
    cuts = [keys * n for n in range(blocks + 1)]
    return cuts[:-1] + [cuts[-1] - keys // 2, cuts[-1]]


def kernel(
    n_st, n_tp, cap, picks, held,
    rate_ref, tok_hbm, wq_hbm, wk_hbm, wv_hbm, wm_hbm, wmk_hbm, wmv_hbm, wg_ref, lift_hbm,
    cos_hbm, sin_hbm, store_hbm, ids_hbm,
    out_ref,
    tok, rows, cos_ref, sin_ref, lift_ref, wq, wk, wv, wm, wmk, wmv, store, slots, landed, ids_s,
    acc_q, acc_k, acc_v, acc_m, acc_g, acc_s, acc_mk, acc_mv,
    rq, rk, rv, mq, ret, gate, xwk, xwv, kv_out, kv_in,
    load_sem, id_send, id_recv, pass_send, pass_recv,
    t_sems, r_sems, w_send, w_own, w_row, w_col, w_final, spread_send, kv_send, kv_recv,
):
    st = lax.axis_index("st")
    me = lax.axis_index("tp")
    z = me // CORES
    core = me % CORES
    n_z = n_tp // CORES
    total, cols = tok.shape[1:]
    heads = mq.shape[1] // MEM_DIM
    mem_cols = mq.shape[1]
    requests = ids_s.shape[1] * ids_s.shape[2]
    blocks = requests // picks
    pass_rows = store.shape[1]
    parts = len(landed)
    per = cap // parts
    chunk = total // PIECES
    block = total // blocks
    keys = picks * pass_rows
    row_cuts = row_bounds(blocks, keys)
    row_pieces = len(row_cuts) - 1
    half = PIECES // 2

    so = jnp.where(z < n_z // 2, -1, 1)
    depth = jnp.minimum(z, n_z - 1 - z)
    edge_z = z + so * depth
    is_edge = depth == 0
    is_helper = depth == 1
    me_out = me + CORES * so
    me_in = me - CORES * so
    pair = me + 1 - 2 * core
    outs = range(1, (n_z - 1) // 2 + 1)
    ins = range(1, n_z)

    loads = []
    pairs = [(store_hbm, store), (ids_hbm, ids_s.at[st]), (tok_hbm, tok.at[me]), (wq_hbm, wq), (wk_hbm, wk),
             (wv_hbm, wv), (wm_hbm, wm), (wmk_hbm, wmk), (wmv_hbm, wmv),
             (cos_hbm, cos_ref), (sin_hbm, sin_ref), (lift_hbm, lift_ref)]
    for i, (src, dst) in enumerate(pairs):
        loads.append(pltpu.make_async_copy(src, dst, load_sem.at[i]))
    loads[1].start()
    loads[0].start()

    barrier = pltpu.get_barrier_semaphore()

    def greet(to_st, to_tp):
        pl.semaphore_signal(barrier, inc=1, device_id=(to_st, to_tp), device_id_type=MESH)

    @pl.when(depth > 0)
    def _():
        greet(st, me_out)
    greet(st, me_in)
    greet(st, pair)
    for d in range(1, n_st):
        greet((st + d) % n_st, me)
    pl.semaphore_wait(barrier, n_st + 1 + (depth > 0).astype(jnp.int32))

    def remote(src, dst, send, recv, to_st, to_tp):
        return pltpu.make_async_remote_copy(
            src_ref=src, dst_ref=dst, send_sem=send, recv_sem=recv,
            device_id=(to_st, to_tp), device_id_type=MESH)

    class Flow:
        def __init__(self, buf, cuts, sems, floor, pair_sem, source=None):
            self.buf, self.floor, self.source, self.pair_sem = buf, floor, source, pair_sem
            self.recv, self.recv_pair, self.send, self.own_out, self.send_pair = sems
            self.cuts = cuts

        def piece(self, j, p):
            return self.buf.at[j, self.rows(p)]

        def rows(self, p):
            return pl.ds(self.cuts[p], self.cuts[p + 1] - self.cuts[p])

        def origin(self, p):
            return self.piece(me, p) if self.source is None else self.source.at[self.rows(p)]

        def along_z(self, j, p, to, src=None, send=None):
            return remote(self.piece(j, p) if src is None else src, self.piece(j, p),
                          self.send.at[j // CORES] if send is None else send, self.recv.at[j // CORES, p], st, to)

        def to_pair(self, j, p, src=None):
            return remote(self.piece(j, p) if src is None else src, self.piece(j, p),
                          self.send_pair.at[0], self.pair_sem(self.recv_pair, j // CORES, p), st, pair)

        def send_own(self, p):
            self.along_z(me, p, me_in, self.origin(p)).start()

            @pl.when(depth > self.floor)
            def _():
                self.along_z(me, p, me_out, self.origin(p), self.own_out.at[0]).start()

        def share_own(self, p):
            self.to_pair(me, p, self.origin(p)).start()

        def at(self, side, d):
            far = CORES * so * d
            if side == OUT:
                return me + far, d <= depth
            return me - far, (d <= n_z - 1 - depth) & (depth >= self.floor)

        def relay(self, side, d, p):
            j, valid = self.at(side, d)

            @pl.when(valid)
            def _():
                self.along_z(j, p, me_in).wait_recv()
                if side == OUT:
                    self.along_z(j, p, me_in).start()
                else:
                    @pl.when(depth > self.floor)
                    def _():
                        self.along_z(j, p, me_out).start()
                self.to_pair(j, p).start()

        def wait_pair(self, ref, sem):
            remote(ref, ref, self.send_pair.at[0], sem, st, pair).wait_recv()

        def drain(self):
            def sent(ref, sem):
                remote(ref, ref, sem, self.recv.at[0, 0], st, me_in).wait_send()
            sent(self.buf.at[0], self.send.at[z])

            @pl.when(depth > self.floor)
            def _():
                sent(self.buf.at[0], self.own_out.at[0])
            for side, distances in ((OUT, outs), (IN, ins)):
                for d in distances:
                    j, valid = self.at(side, d)

                    @pl.when(valid if side == OUT else valid & (depth > self.floor))
                    def _():
                        sent(self.buf.at[0], self.send.at[j // CORES])

            @pl.when(depth >= self.floor)
            def _():
                sent(self.buf.at[pl.ds(0, n_z)], self.send_pair.at[0])

            @pl.when(depth < self.floor)
            def _():
                sent(self.buf.at[0], self.send_pair.at[0])

    toks = Flow(tok, [chunk * p for p in range(PIECES + 1)], t_sems, 0, lambda sems, chip, p: sems.at[chip, p // half], tok_hbm)
    passes = Flow(rows, row_cuts, r_sems, 1, lambda sems, chip, p: sems.at[p])

    n_b = square_split(n_st)
    n_a = n_st // n_b
    a, b = st // n_b, st % n_b
    row_mates = [a * n_b + (b + i) % n_b for i in range(1, n_b)]
    col_mates = [(a + i) % n_a * n_b + b for i in range(1, n_a)]
    mates = row_mates + col_mates
    along_row = range(0, n_b - 1)
    along_col = range(n_b - 1, len(mates))
    sub = CORES * cols // n_st // 2
    others = n_z - 1
    lent = 2 * others
    xw = (xwk, xwv)

    def lent_at(e, part, s, count=1):
        start = (edge_z - so * (e + 1)) * (CORES * cols) + (2 * s + part) * sub
        return pl.ds(pl.multiple_of(start, sub), sub * count)

    def lend(w):
        kv, e = w // others, w % others
        at = lent_at(e, 0, st, 2)
        return remote((wmk_hbm, wmv_hbm)[kv].at[at], xw[kv].at[at], w_send.at[0], w_own.at[w], st, me_in)

    def lend_all(first, last):
        for w in range(first, last):
            lend(w).start()

    def spread(w, part, s, i, send, recv):
        kv, e = w // others, w % others
        here = xw[kv].at[lent_at(e, part, s)]
        return remote(here, here, spread_send.at[send], recv, mates[i], me)

    def spread_own(first, last):
        @pl.when(is_helper)
        def _():
            for w in range(first, last):
                lend(w).wait_recv()
                for part in range(2):
                    for i in along_row:
                        recv = w_row.at[w, n_b - 2 - i] if part == 0 else w_final.at[w // others]
                        spread(w, part, st, i, 0, recv).start()
                    for i in along_col:
                        recv = w_col.at[w, n_a - 2 - (i - (n_b - 1))] if part == 1 else w_final.at[w // others]
                        spread(w, part, st, i, 0, recv).start()

    def spread_on(first, last):
        @pl.when(is_helper)
        def _():
            for w in range(first, last):
                final = w_final.at[w // others]
                for k, s in enumerate(row_mates):
                    spread(w, 0, s, 0, 1, w_row.at[w, k]).wait_recv()
                    for i in along_col:
                        spread(w, 0, s, i, 1, final).start()
                for k, s in enumerate(col_mates):
                    spread(w, 1, s, 0, 1, w_col.at[w, k]).wait_recv()
                    for i in along_row:
                        spread(w, 1, s, i, 1, final).start()

    def lent_rows(count):
        return xwk.at[pl.ds(0, count * sub)]

    def spread_last(kv):
        @pl.when(is_helper)
        def _():
            whole = lent_rows(others * (n_b * (n_a - 1) + n_a * (n_b - 1)))
            remote(whole, whole, spread_send.at[0], w_final.at[kv], st, me_in).wait_recv()

    def spread_drain():
        for k, count in enumerate((2 * len(mates), 2 * (n_a - 1) * (n_b - 1))):
            whole = lent_rows(2 * others * count)
            remote(whole, whole, spread_send.at[k], w_final.at[0], st, me_in).wait_send()

    def lend_drain():
        whole = lent_rows(2 * others * 2)
        remote(whole, whole, w_send.at[0], w_own.at[0], st, me_in).wait_send()

    def kv_copy(kv, p):
        at = passes.rows(p)
        return remote(kv_out.at[kv, at], kv_in.at[kv, at], kv_send.at[0], kv_recv.at[kv, p], st, me_out)

    def id_copy(d):
        return remote(ids_s.at[st], ids_s.at[st], id_send.at[d], id_recv.at[st], (st + d) % n_st, me)

    def id_wait(d):
        other = (st + d) % n_st
        return remote(ids_s.at[other], ids_s.at[other], id_send.at[d], id_recv.at[other], other, me)

    loads[1].wait()
    for d in range(1, n_st):
        id_copy(d).start()

    @pl.when(is_edge)
    def _():
        for p in range(half):
            lend_all(p, p + 1)
            toks.send_own(p)
        lend_all(half, others)
        toks.send_own(half)

    @pl.when(depth > 0)
    def _():
        for p in range(PIECES):
            toks.send_own(p)
    for p in range(PIECES):
        toks.share_own(p)
    loads[2].start()

    for ref in (acc_q, acc_k, acc_v, acc_m, acc_g, acc_s):
        ref[...] = jnp.zeros_like(ref)

    for d in range(1, n_st):
        id_wait(d).wait_recv()
    loads[0].wait()
    for i in range(3, len(pairs)):
        loads[i].start()

    def asked(source, k):
        found = jnp.int32(0)
        seen = jnp.int32(0)
        for i in range(requests):
            ident = ids_s[source, i % picks, i // picks]
            mine = (ident // held) == st
            found = jnp.where(mine & (seen == k), ident % held, found)
            seen = seen + mine.astype(jnp.int32)
        return found

    def pass_copy(g, d):
        return remote(slots.at[d, pl.ds(g * per, per)], landed[g].at[st], pass_send.at[0], pass_recv.at[g],
                      (st + d) % n_st, me)

    def pass_waits(first, last):
        for g in range(first, last):
            all_of = landed[g].at[pl.ds(0, n_st - 1)]
            remote(all_of, all_of, pass_send.at[0], pass_recv.at[g], (st + 1) % n_st, me).wait_recv()

    for g in range(parts):
        def fill(d, carry):
            for k in range(g * per, (g + 1) * per):
                slots[d, k] = store[asked((st + d) % n_st, k)]
            return carry
        lax.fori_loop(1, n_st, fill, 0)
        for d in range(1, n_st):
            pass_copy(g, d).start()
    for k in range(cap):
        landed[k // per][st, k % per] = store[asked(st, k)]

    def build(block):
        reach = min(parts, -(-picks * (block + 1) // per))
        for i in range(block * picks, (block + 1) * picks):
            ident = ids_s[st, i % picks, i // picks]
            owner = ident // held
            order = jnp.int32(0)
            for e in range(i):
                order = order + ((ids_s[st, e % picks, e // picks] // held) == owner).astype(jnp.int32)
            value = landed[0][owner, jnp.minimum(order, per - 1)]
            for g in range(1, reach):
                other = landed[g][owner, jnp.clip(order - g * per, 0, per - 1)]
                value = jnp.where(order >= g * per, other, value)
            rows[me, pl.ds(i * pass_rows, pass_rows), :] = value

    def take_tokens(at_z, h):
        here = pl.ds(pl.multiple_of(h * (half * chunk), half * chunk), half * chunk)
        xs, ats = [], []
        for c in range(CORES):
            j = at_z * CORES + c
            xs.append(tok[j, here, :])
            ats.append(pl.ds(pl.multiple_of(j * cols, cols), cols))
        for acc, w in ((acc_q, wq), (acc_k, wk), (acc_v, wv), (acc_m, wm)):
            acc[here, :] += sum(dot(x, w[at, :]) for x, at in zip(xs, ats))
        squares = acc_s[here, :]
        for x, at in zip(xs, ats):
            wide = x.astype(F32)
            if heads > 1:
                acc_g[here, :] += dot_nt(x, wg_ref[:, at])
            else:
                acc_g[here, :] += jnp.sum(wide * wg_ref[:, at].astype(F32), axis=1, keepdims=True)
            for piece in range(cols // 128):
                slab = wide[:, piece * 128:(piece + 1) * 128]
                squares = squares + slab * slab
        acc_s[here, :] = squares

    def tokens_of(side, d, h):
        j, valid = toks.at(side, d)

        def go():
            toks.wait_pair(tok.at[j + 1 - 2 * core, pl.ds(h * half * chunk, half * chunk)],
                           toks.recv_pair.at[j // CORES, h])
            take_tokens(j // CORES, h)
        if d == 0:
            go()
        else:
            pl.when(valid)(go)

    def rows_wait(p, chips):
        passes.wait_pair(rows.at[pl.ds(0, chips), passes.rows(p)], passes.recv_pair.at[p])

    def project(at, base, count, w):
        total_of = None
        for q in range(count):
            j = base + q
            part = dot(rows[j, at, :], w[pl.ds(pl.multiple_of(j * cols, cols), cols), :])
            total_of = part if total_of is None else total_of + part
        return total_of

    def rows_all(n, base, count):
        at = pl.ds(n * keys, keys)
        acc_mk[at, :] = project(at, base, count, wmk)
        acc_mv[at, :] = project(at, base, count, wmv)

    def prepare(c, carry):
        here = pl.ds(pl.multiple_of(c * chunk, chunk), chunk)
        scale = lax.rsqrt(jnp.sum(acc_s[here, :], axis=1, keepdims=True) / (n_tp * cols) + NORM_EPS)
        cosine, sine = cos_ref[here, :], sin_ref[here, :]

        def rotate(v):
            return v * cosine + pltpu.roll(v, KEY_DIM // 2, 1) * sine
        for h in range(heads):
            at = slice(h * KEY_DIM, (h + 1) * KEY_DIM)
            rq[here, at] = rotate(acc_q[here, at] * scale).astype(BF16)
            rk[here, at] = (rotate(acc_k[here, at] * scale) * KEY_DIM ** (-0.5)).astype(BF16)
            m = acc_m[here, at]
            mq[here, at] = (m * lax.rsqrt(jnp.mean(m * m, axis=1, keepdims=True) + NORM_EPS)).astype(BF16)
        rv[here, :] = (acc_v[here, :] * scale).astype(BF16)
        gate[here, :] = jax.nn.sigmoid(acc_g[here, :] * scale)
        return carry

    def retain(c):
        here = pl.ds(c * chunk, chunk)
        start = (c * chunk) // SEQ_LEN * SEQ_LEN
        length = (c + 1) * chunk - start
        whole = pl.ds(start, length)
        t = lax.broadcasted_iota(jnp.int32, (chunk, length), 0) + (c * chunk - start)
        s = lax.broadcasted_iota(jnp.int32, (chunk, length), 1)
        gap = (t - s).astype(F32)
        for h in range(heads):
            at = slice(h * KEY_DIM, (h + 1) * KEY_DIM)
            wide = slice(h * VALUE_DIM, (h + 1) * VALUE_DIM)
            decay = jnp.where(gap >= 0.0, jnp.exp(-rate_ref[h] * jnp.maximum(gap, 0.0)), 0.0)
            scores = dot_nt(rq[here, at], rk[whole, at]) * decay
            upper = scores.astype(BF16)
            lower = (scores - upper.astype(F32)).astype(BF16)
            value = rv[whole, wide]
            o = dot(upper, value) + dot(lower, value)
            o = o - jnp.mean(o, axis=1, keepdims=True)
            ret[here, wide] = o * lax.rsqrt(jnp.mean(o * o, axis=1, keepdims=True) + NORM_EPS)

    def assist(kv, p):
        @pl.when(is_helper)
        def _():
            at = passes.rows(p)
            base = jnp.where(so < 0, CORES, 0)
            kv_out[kv, at, :] = project(at, base, CORES * others, xw[kv]).astype(BF16)
            kv_copy(kv, p).start()

    def attend_keys(n):
        here, there = pl.ds(n * block, block), pl.ds(n * keys, keys)
        state = []
        for h in range(heads):
            at = slice(h * MEM_DIM, (h + 1) * MEM_DIM)
            k = acc_mk[there, at]
            k = (k * lax.rsqrt(jnp.mean(k * k, axis=1, keepdims=True) + NORM_EPS)).astype(BF16)
            exponent = jnp.exp(dot_nt(mq[here, at], k) * MEM_DIM ** (-0.5))
            state.append((exponent.astype(BF16), jnp.sum(exponent, axis=1, keepdims=True)))
        return state

    def attend_values(n, state):
        here, there = pl.ds(n * block, block), pl.ds(n * keys, keys)
        for h in range(heads):
            at = slice(h * MEM_DIM, (h + 1) * MEM_DIM)
            wide = slice(h * VALUE_DIM, (h + 1) * VALUE_DIM)
            exponent, mass = state[h]
            v = acc_mv[there, at].astype(BF16)
            o = (dot(exponent, v) / mass).astype(BF16)
            lifted = dot(o, lift_ref[h])
            out_ref[here, wide] = (ret[here, wide] + gate[here, h:h + 1] * lifted).astype(BF16)

    def attend(n):
        attend_values(n, attend_keys(n))

    def returned(kv, n):
        for p in range(row_pieces):
            if n * keys <= row_cuts[p] < (n + 1) * keys:
                at = passes.rows(p)
                kv_copy(kv, p).wait_recv()
                acc = (acc_mk, acc_mv)[kv]
                acc[at, :] += kv_in[kv, at, :].astype(F32)

    def load_waits():
        for i in range(2, len(pairs)):
            loads[i].wait()

    def settle(c):
        prepare(c, 0)
        retain(c)

    early_parts = min(parts, -(-picks // per))

    def in_tokens(p, distances):
        for d in distances:
            toks.relay(IN, d, p)

    def out_tokens(p):
        for d in outs:
            toks.relay(OUT, d, p)

    def in_rows(p, distances):
        for d in distances:
            passes.relay(IN, d, p)

    def out_rows(p):
        for d in outs:
            passes.relay(OUT, d, p)

    near, far = ins[:1], ins[1:]
    last = blocks - 1

    @pl.when(is_edge)
    def _():
        in_tokens(0, near)
        in_tokens(1, near)
        pass_waits(0, early_parts)
        build(0)
        passes.send_own(0)
        passes.share_own(0)
        for p in range(half + 1, PIECES):
            toks.send_own(p)
        lend_all(others, lent - 1)
        in_tokens(2, near)
        load_waits()
        tokens_of(IN, 0, 0)
        in_tokens(3, near)
        pass_waits(early_parts, parts)
        for n in range(1, blocks):
            build(n)
        for p in range(1, row_pieces):
            passes.send_own(p)
            passes.share_own(p)
            if p == 1:
                lend_all(lent - 1, lent)
        tokens_of(IN, 0, 1)
        in_tokens(0, ins[1:2])
        tokens_of(IN, 1, 0)
        in_tokens(1, ins[1:2])
        tokens_of(IN, 1, 1)
        in_tokens(2, ins[1:2])
        tokens_of(IN, 2, 0)
        in_tokens(3, ins[1:2])
        tokens_of(IN, 2, 1)
        for p in range(row_pieces):
            rows_wait(p, 1)
        for n in range(blocks):
            rows_all(n, z * CORES, CORES)
        for d in ins[2:]:
            in_tokens(0, [d])
            in_tokens(1, [d])
            tokens_of(IN, d, 0)
        settle(0)
        settle(1)
        for d in ins[2:]:
            in_tokens(2, [d])
            in_tokens(3, [d])
            tokens_of(IN, d, 1)
        settle(2)
        settle(3)
        for n in range(blocks):
            returned(0, n)
            state = attend_keys(n)
            returned(1, n)
            attend_values(n, state)
        lend_drain()

    @pl.when(depth > 0)
    def _():
        in_tokens(0, near)
        spread_own(0, 1)
        in_tokens(1, near)
        out_tokens(0)
        in_tokens(2, near)
        spread_own(1, 2)
        pass_waits(0, early_parts)
        build(0)
        passes.send_own(0)
        passes.share_own(0)
        in_tokens(3, near)
        out_tokens(1)
        load_waits()
        tokens_of(IN, 0, 0)
        in_tokens(0, far)
        spread_own(2, others)
        pass_waits(early_parts, parts)
        for n in range(1, blocks):
            build(n)
        for p in range(1, row_pieces):
            passes.share_own(p)
        tokens_of(IN, 0, 1)
        out_tokens(2)
        passes.send_own(1)
        in_rows(0, near)
        tokens_of(IN, 1, 0)
        in_tokens(1, far)
        out_rows(0)
        tokens_of(IN, 1, 1)
        for d in outs:
            tokens_of(OUT, d, 0)
        in_tokens(2, far)
        out_tokens(3)
        passes.send_own(2)
        spread_on(0, others - 1)
        for d in far:
            tokens_of(IN, d, 0)
        spread_on(others - 1, others)
        in_rows(1, near)
        spread_own(others, lent - 2)
        settle(0)
        settle(1)
        spread_own(lent - 2, lent - 1)
        in_rows(0, far)
        rows_wait(0, n_z)
        spread_last(0)
        assist(0, 0)
        in_tokens(3, far)
        out_rows(1)
        for p in range(last, row_pieces):
            passes.send_own(p)
        spread_on(others, lent - 2)
        for d in outs:
            tokens_of(OUT, d, 1)
        in_rows(2, near)
        spread_own(lent - 1, lent)
        spread_on(lent - 2, lent - 1)
        for d in far:
            tokens_of(IN, d, 1)
        out_rows(2)
        in_rows(1, far)
        settle(2)
        spread_on(lent - 1, lent)
        out_rows(3)
        rows_wait(1, n_z)
        assist(0, 1)
        out_rows(4)
        in_rows(last, near)
        spread_last(1)
        assist(1, 0)
        assist(1, 1)
        in_rows(2, far)
        settle(3)
        in_rows(3, far)
        rows_wait(2, n_z)
        assist(0, 2)
        assist(1, 2)
        in_rows(4, near)
        in_rows(4, far)
        rows_wait(3, n_z)
        assist(0, 3)
        assist(1, 3)
        rows_wait(4, n_z)
        assist(0, 4)
        assist(1, 4)
        for n in range(blocks):
            rows_all(n, 0, n_tp)
            attend(n)

        @pl.when(is_helper)
        def _():
            spread_drain()
            remote(kv_out, kv_in, kv_send.at[0], kv_recv.at[0, 0], st, me_out).wait_send()

    for d in range(1, n_st):
        id_copy(d).wait_send()
    all_slots = slots.at[pl.ds(1, n_st - 1)]
    remote(all_slots, all_slots, pass_send.at[0], pass_recv.at[0], (st + 1) % n_st, me).wait_send()
    toks.drain()
    passes.drain()


def rotary_tables(total):
    half = KEY_DIM // 2
    angle = (np.arange(total) % SEQ_LEN)[:, None] * ROPE_BASE ** (-np.arange(half) / half)[None, :]
    cosine, sine = np.cos(angle), np.sin(angle)
    return (np.concatenate([cosine, cosine], 1).astype(np.float32),
            np.concatenate([-sine, sine], 1).astype(np.float32))


def solution(mesh):
    n_st, n_tp = mesh.shape["st"], mesh.shape["tp"]
    n_z = n_tp // CORES
    assert n_z >= 4

    def per_device(tokens, w_query, w_key, w_value, w_mem_query, w_mem_key, w_mem_value, w_gate, w_lift,
                   decay_rate, store, passage_ids):
        total, cols = tokens.shape
        heads = decay_rate.shape[0]
        blocks, picks = passage_ids.shape
        requests = blocks * picks
        held, pass_rows, _ = store.shape
        cap = max(1, 2 * requests // n_st)
        parts = cap // picks if cap % picks == 0 else 1
        cosine, sine = rotary_tables(total)
        hbm = pl.BlockSpec(memory_space=pl.ANY)
        vmem = pl.BlockSpec(memory_space=pltpu.VMEM)
        smem = pl.BlockSpec(memory_space=pltpu.SMEM)
        V = pltpu.VMEM
        dma = pltpu.SemaphoreType.DMA
        wide = w_value.shape[1]
        key_cols, mem_cols = w_query.shape[1], w_mem_query.shape[1]
        n_b = square_split(n_st)

        row_pieces = len(row_bounds(blocks, picks * pass_rows)) - 1

        def flow_sems(pieces, *pair_shape):
            return dma((n_z, pieces)), dma(pair_shape), dma((n_z,)), dma((1,)), dma((1,))
        all_rows = requests * pass_rows
        scratch = [
            V((n_tp, total, cols), BF16), V((n_tp, all_rows, cols), BF16),
            V(cosine.shape, F32), V(sine.shape, F32), V(w_lift.shape, BF16),
            V(w_query.shape, BF16), V(w_key.shape, BF16), V(w_value.shape, BF16),
            V(w_mem_query.shape, BF16), V(w_mem_key.shape, BF16), V(w_mem_value.shape, BF16),
            V(store.shape, BF16), V((n_st, cap, pass_rows, cols), BF16),
            tuple(V((n_st, cap // parts, pass_rows, cols), BF16) for _ in range(parts)),
            pltpu.SMEM((n_st, picks, blocks), jnp.int32),
            V((total, key_cols), F32), V((total, key_cols), F32), V((total, wide), F32), V((total, mem_cols), F32),
            V((total, heads), F32), V((total, 128), F32),
            V((all_rows, mem_cols), F32), V((all_rows, mem_cols), F32),
            V((total, key_cols), BF16), V((total, key_cols), BF16), V((total, wide), BF16), V((total, mem_cols), BF16),
            V((total, wide), F32), V((total, heads), F32),
            V(w_mem_key.shape, BF16), V(w_mem_value.shape, BF16),
            V((2, all_rows, mem_cols), BF16), V((2, all_rows, mem_cols), BF16),
            dma((13,)), dma((n_st,)), dma((n_st,)), dma((1,)), dma((parts,)),
            flow_sems(PIECES, n_z, 2), flow_sems(row_pieces, row_pieces),
            dma((1,)), dma((2 * (n_z - 1),)), dma((2 * (n_z - 1), n_b - 1)), dma((2 * (n_z - 1), n_st // n_b - 1)),
            dma((2,)), dma((2,)), dma((1,)), dma((2, row_pieces)),
        ]
        return pl.pallas_call(
            functools.partial(kernel, n_st, n_tp, cap, picks, held),
            out_shape=pltpu.VMEM((total, heads * VALUE_DIM), BF16),
            in_specs=[smem] + [hbm] * 7 + [vmem] + [hbm] * 5,
            out_specs=vmem,
            scratch_shapes=scratch,
            compiler_params=pltpu.CompilerParams(
                collective_id=0, has_side_effects=True, vmem_limit_bytes=60 * 1024 * 1024),
        )(decay_rate, tokens, w_query, w_key, w_value, w_mem_query, w_mem_key, w_mem_value,
          w_gate.T, w_lift, jnp.asarray(cosine), jnp.asarray(sine), store, passage_ids.T)

    in_specs = (P("st", "tp"),) + (P(None, "tp"),) * 7 + (
        P("tp", None, None), P("tp"), P("st", None, "tp"), P("st", None))
    return jax.shard_map(per_device, mesh=mesh, in_specs=in_specs, out_specs=P("st", "tp"), check_vma=False)
```

```python
import functools

import jax
import jax.numpy as jnp
import numpy as np
from jax import lax
from jax.experimental import pallas as pl
from jax.experimental.pallas import tpu as pltpu
from jax.sharding import PartitionSpec as P

KEY_DIM = 128
VALUE_DIM = 256
MEM_DIM = 128
SEQ_LEN = 512
NORM_EPS = 1e-06
ROPE_BASE = 10000.0
CORES = 2
PIECES = 4
OUT, IN = 0, 1
MESH = pl.DeviceIdType.MESH
F32 = jnp.float32
BF16 = jnp.bfloat16


def dot(a, b):
    return jnp.dot(a, b, preferred_element_type=F32)


def dot_nt(a, b):
    return lax.dot_general(a, b, (((1,), (1,)), ((), ())), preferred_element_type=F32)


def square_split(n):
    return 1 << ((n.bit_length() - 1) // 2)


def row_bounds(blocks, keys):
    cuts = [keys * n for n in range(blocks + 1)]
    return cuts[:-1] + [cuts[-1] - keys // 2, cuts[-1]]


def kernel(
    n_st, n_tp, cap, picks, held,
    rate_ref, tok_hbm, wq_hbm, wk_hbm, wv_hbm, wm_hbm, wmk_hbm, wmv_hbm, wg_ref, lift_hbm,
    cos_hbm, sin_hbm, store_hbm, ids_hbm,
    out_ref,
    tok, rows, cos_ref, sin_ref, lift_ref, wq, wk, wv, wm, wmk, wmv, store, slots, landed, ids_s,
    acc_q, acc_k, acc_v, acc_m, acc_g, acc_s, acc_mk, acc_mv,
    rq, rk, rv, mq, ret, gate, xwk, xwv, kv_out, kv_in,
    load_sem, id_send, id_recv, pass_send, pass_recv,
    t_sems, r_sems, w_send, w_own, w_row, w_col, w_final, spread_send, kv_send, kv_recv,
):
    st = lax.axis_index("st")
    me = lax.axis_index("tp")
    z = me // CORES
    core = me % CORES
    n_z = n_tp // CORES
    total, cols = tok.shape[1:]
    heads = mq.shape[1] // MEM_DIM
    mem_cols = mq.shape[1]
    requests = ids_s.shape[1] * ids_s.shape[2]
    blocks = requests // picks
    pass_rows = store.shape[1]
    parts = len(landed)
    per = cap // parts
    chunk = total // PIECES
    block = total // blocks
    keys = picks * pass_rows
    row_cuts = row_bounds(blocks, keys)
    row_pieces = len(row_cuts) - 1
    half = PIECES // 2

    so = jnp.where(z < n_z // 2, -1, 1)
    depth = jnp.minimum(z, n_z - 1 - z)
    edge_z = z + so * depth
    is_edge = depth == 0
    is_helper = depth == 1
    me_out = me + CORES * so
    me_in = me - CORES * so
    pair = me + 1 - 2 * core
    outs = range(1, (n_z - 1) // 2 + 1)
    ins = range(1, n_z)

    loads = []
    pairs = [(store_hbm, store), (ids_hbm, ids_s.at[st]), (tok_hbm, tok.at[me]), (wq_hbm, wq), (wk_hbm, wk),
             (wv_hbm, wv), (wm_hbm, wm), (wmk_hbm, wmk), (wmv_hbm, wmv),
             (cos_hbm, cos_ref), (sin_hbm, sin_ref), (lift_hbm, lift_ref)]
    for i, (src, dst) in enumerate(pairs):
        loads.append(pltpu.make_async_copy(src, dst, load_sem.at[i]))
    loads[1].start()
    loads[0].start()

    barrier = pltpu.get_barrier_semaphore()

    def greet(to_st, to_tp):
        pl.semaphore_signal(barrier, inc=1, device_id=(to_st, to_tp), device_id_type=MESH)

    @pl.when(depth > 0)
    def _():
        greet(st, me_out)
    greet(st, me_in)
    greet(st, pair)
    for d in range(1, n_st):
        greet((st + d) % n_st, me)
    pl.semaphore_wait(barrier, n_st + 1 + (depth > 0).astype(jnp.int32))

    def remote(src, dst, send, recv, to_st, to_tp):
        return pltpu.make_async_remote_copy(
            src_ref=src, dst_ref=dst, send_sem=send, recv_sem=recv,
            device_id=(to_st, to_tp), device_id_type=MESH)

    class Flow:
        def __init__(self, buf, cuts, sems, floor, pair_sem, source=None):
            self.buf, self.floor, self.source, self.pair_sem = buf, floor, source, pair_sem
            self.recv, self.recv_pair, self.send, self.own_out, self.send_pair = sems
            self.cuts = cuts

        def piece(self, j, p):
            return self.buf.at[j, self.rows(p)]

        def rows(self, p):
            return pl.ds(self.cuts[p], self.cuts[p + 1] - self.cuts[p])

        def origin(self, p):
            return self.piece(me, p) if self.source is None else self.source.at[self.rows(p)]

        def along_z(self, j, p, to, src=None, send=None):
            return remote(self.piece(j, p) if src is None else src, self.piece(j, p),
                          self.send.at[j // CORES] if send is None else send, self.recv.at[j // CORES, p], st, to)

        def to_pair(self, j, p, src=None):
            return remote(self.piece(j, p) if src is None else src, self.piece(j, p),
                          self.send_pair.at[0], self.pair_sem(self.recv_pair, j // CORES, p), st, pair)

        def send_own(self, p):
            self.along_z(me, p, me_in, self.origin(p)).start()

            @pl.when(depth > self.floor)
            def _():
                self.along_z(me, p, me_out, self.origin(p), self.own_out.at[0]).start()

        def share_own(self, p):
            self.to_pair(me, p, self.origin(p)).start()

        def at(self, side, d):
            far = CORES * so * d
            if side == OUT:
                return me + far, d <= depth
            return me - far, (d <= n_z - 1 - depth) & (depth >= self.floor)

        def relay(self, side, d, p):
            j, valid = self.at(side, d)

            @pl.when(valid)
            def _():
                self.along_z(j, p, me_in).wait_recv()
                if side == OUT:
                    self.along_z(j, p, me_in).start()
                else:
                    @pl.when(depth > self.floor)
                    def _():
                        self.along_z(j, p, me_out).start()
                self.to_pair(j, p).start()

        def wait_pair(self, ref, sem):
            remote(ref, ref, self.send_pair.at[0], sem, st, pair).wait_recv()

        def drain(self):
            def sent(ref, sem):
                remote(ref, ref, sem, self.recv.at[0, 0], st, me_in).wait_send()
            sent(self.buf.at[0], self.send.at[z])

            @pl.when(depth > self.floor)
            def _():
                sent(self.buf.at[0], self.own_out.at[0])
            for side, distances in ((OUT, outs), (IN, ins)):
                for d in distances:
                    j, valid = self.at(side, d)

                    @pl.when(valid if side == OUT else valid & (depth > self.floor))
                    def _():
                        sent(self.buf.at[0], self.send.at[j // CORES])

            @pl.when(depth >= self.floor)
            def _():
                sent(self.buf.at[pl.ds(0, n_z)], self.send_pair.at[0])

            @pl.when(depth < self.floor)
            def _():
                sent(self.buf.at[0], self.send_pair.at[0])

    toks = Flow(tok, [chunk * p for p in range(PIECES + 1)], t_sems, 0, lambda sems, chip, p: sems.at[chip, p // half], tok_hbm)
    passes = Flow(rows, row_cuts, r_sems, 1, lambda sems, chip, p: sems.at[p])

    n_b = square_split(n_st)
    n_a = n_st // n_b
    a, b = st // n_b, st % n_b
    row_mates = [a * n_b + (b + i) % n_b for i in range(1, n_b)]
    col_mates = [(a + i) % n_a * n_b + b for i in range(1, n_a)]
    mates = row_mates + col_mates
    along_row = range(0, n_b - 1)
    along_col = range(n_b - 1, len(mates))
    sub = CORES * cols // n_st // 2
    others = n_z - 1
    lent = 2 * others
    xw = (xwk, xwv)

    def lent_at(e, part, s, count=1):
        start = (edge_z - so * (e + 1)) * (CORES * cols) + (2 * s + part) * sub
        return pl.ds(pl.multiple_of(start, sub), sub * count)

    def lend(w):
        kv, e = w // others, w % others
        at = lent_at(e, 0, st, 2)
        return remote((wmk_hbm, wmv_hbm)[kv].at[at], xw[kv].at[at], w_send.at[0], w_own.at[w], st, me_in)

    def lend_all(first, last):
        for w in range(first, last):
            lend(w).start()

    def spread(w, part, s, i, send, recv):
        kv, e = w // others, w % others
        here = xw[kv].at[lent_at(e, part, s)]
        return remote(here, here, spread_send.at[send], recv, mates[i], me)

    def spread_own(first, last):
        @pl.when(is_helper)
        def _():
            for w in range(first, last):
                lend(w).wait_recv()
                for part in range(2):
                    for i in along_row:
                        recv = w_row.at[w, n_b - 2 - i] if part == 0 else w_final.at[w // others]
                        spread(w, part, st, i, 0, recv).start()
                    for i in along_col:
                        recv = w_col.at[w, n_a - 2 - (i - (n_b - 1))] if part == 1 else w_final.at[w // others]
                        spread(w, part, st, i, 0, recv).start()

    def spread_on(first, last):
        @pl.when(is_helper)
        def _():
            for w in range(first, last):
                final = w_final.at[w // others]
                for k, s in enumerate(row_mates):
                    spread(w, 0, s, 0, 1, w_row.at[w, k]).wait_recv()
                    for i in along_col:
                        spread(w, 0, s, i, 1, final).start()
                for k, s in enumerate(col_mates):
                    spread(w, 1, s, 0, 1, w_col.at[w, k]).wait_recv()
                    for i in along_row:
                        spread(w, 1, s, i, 1, final).start()

    def lent_rows(count):
        return xwk.at[pl.ds(0, count * sub)]

    def spread_last(kv):
        @pl.when(is_helper)
        def _():
            whole = lent_rows(others * (n_b * (n_a - 1) + n_a * (n_b - 1)))
            remote(whole, whole, spread_send.at[0], w_final.at[kv], st, me_in).wait_recv()

    def spread_drain():
        for k, count in enumerate((2 * len(mates), 2 * (n_a - 1) * (n_b - 1))):
            whole = lent_rows(2 * others * count)
            remote(whole, whole, spread_send.at[k], w_final.at[0], st, me_in).wait_send()

    def lend_drain():
        whole = lent_rows(2 * others * 2)
        remote(whole, whole, w_send.at[0], w_own.at[0], st, me_in).wait_send()

    def kv_copy(kv, p):
        at = passes.rows(p)
        return remote(kv_out.at[kv, at], kv_in.at[kv, at], kv_send.at[0], kv_recv.at[kv, p], st, me_out)

    def id_copy(d):
        return remote(ids_s.at[st], ids_s.at[st], id_send.at[d], id_recv.at[st], (st + d) % n_st, me)

    def id_wait(d):
        other = (st + d) % n_st
        return remote(ids_s.at[other], ids_s.at[other], id_send.at[d], id_recv.at[other], other, me)

    loads[1].wait()
    for d in range(1, n_st):
        id_copy(d).start()

    @pl.when(is_edge)
    def _():
        for p in range(half):
            lend_all(p, p + 1)
            toks.send_own(p)
        lend_all(half, others)
        toks.send_own(half)

    @pl.when(depth > 0)
    def _():
        for p in range(PIECES):
            toks.send_own(p)
    for p in range(PIECES):
        toks.share_own(p)
    loads[2].start()

    for ref in (acc_q, acc_k, acc_v, acc_m, acc_g, acc_s):
        ref[...] = jnp.zeros_like(ref)

    for d in range(1, n_st):
        id_wait(d).wait_recv()
    loads[0].wait()
    for i in range(3, len(pairs)):
        loads[i].start()

    def asked(source, k):
        found = jnp.int32(0)
        seen = jnp.int32(0)
        for i in range(requests):
            ident = ids_s[source, i % picks, i // picks]
            mine = (ident // held) == st
            found = jnp.where(mine & (seen == k), ident % held, found)
            seen = seen + mine.astype(jnp.int32)
        return found

    def pass_copy(g, d):
        return remote(slots.at[d, pl.ds(g * per, per)], landed[g].at[st], pass_send.at[0], pass_recv.at[g],
                      (st + d) % n_st, me)

    def pass_waits(first, last):
        for g in range(first, last):
            all_of = landed[g].at[pl.ds(0, n_st - 1)]
            remote(all_of, all_of, pass_send.at[0], pass_recv.at[g], (st + 1) % n_st, me).wait_recv()

    for g in range(parts):
        def fill(d, carry):
            for k in range(g * per, (g + 1) * per):
                slots[d, k] = store[asked((st + d) % n_st, k)]
            return carry
        lax.fori_loop(1, n_st, fill, 0)
        for d in range(1, n_st):
            pass_copy(g, d).start()
    for k in range(cap):
        landed[k // per][st, k % per] = store[asked(st, k)]

    def build(block):
        reach = min(parts, -(-picks * (block + 1) // per))
        for i in range(block * picks, (block + 1) * picks):
            ident = ids_s[st, i % picks, i // picks]
            owner = ident // held
            order = jnp.int32(0)
            for e in range(i):
                order = order + ((ids_s[st, e % picks, e // picks] // held) == owner).astype(jnp.int32)
            value = landed[0][owner, jnp.minimum(order, per - 1)]
            for g in range(1, reach):
                other = landed[g][owner, jnp.clip(order - g * per, 0, per - 1)]
                value = jnp.where(order >= g * per, other, value)
            rows[me, pl.ds(i * pass_rows, pass_rows), :] = value

    def take_tokens(at_z, h):
        here = pl.ds(pl.multiple_of(h * (half * chunk), half * chunk), half * chunk)
        xs, ats = [], []
        for c in range(CORES):
            j = at_z * CORES + c
            xs.append(tok[j, here, :])
            ats.append(pl.ds(pl.multiple_of(j * cols, cols), cols))
        for acc, w in ((acc_q, wq), (acc_k, wk), (acc_v, wv), (acc_m, wm)):
            acc[here, :] += sum(dot(x, w[at, :]) for x, at in zip(xs, ats))
        squares = acc_s[here, :]
        for x, at in zip(xs, ats):
            wide = x.astype(F32)
            if heads > 1:
                acc_g[here, :] += dot_nt(x, wg_ref[:, at])
            else:
                acc_g[here, :] += jnp.sum(wide * wg_ref[:, at].astype(F32), axis=1, keepdims=True)
            for piece in range(cols // 128):
                slab = wide[:, piece * 128:(piece + 1) * 128]
                squares = squares + slab * slab
        acc_s[here, :] = squares

    def tokens_of(side, d, h):
        j, valid = toks.at(side, d)

        def go():
            toks.wait_pair(tok.at[j + 1 - 2 * core, pl.ds(h * half * chunk, half * chunk)],
                           toks.recv_pair.at[j // CORES, h])
            take_tokens(j // CORES, h)
        if d == 0:
            go()
        else:
            pl.when(valid)(go)

    def rows_wait(p, chips):
        passes.wait_pair(rows.at[pl.ds(0, chips), passes.rows(p)], passes.recv_pair.at[p])

    def project(at, base, count, w):
        total_of = None
        for q in range(count):
            j = base + q
            part = dot(rows[j, at, :], w[pl.ds(pl.multiple_of(j * cols, cols), cols), :])
            total_of = part if total_of is None else total_of + part
        return total_of

    def rows_all(n, base, count):
        at = pl.ds(n * keys, keys)
        acc_mk[at, :] = project(at, base, count, wmk)
        acc_mv[at, :] = project(at, base, count, wmv)

    def prepare(c, carry):
        here = pl.ds(pl.multiple_of(c * chunk, chunk), chunk)
        scale = lax.rsqrt(jnp.sum(acc_s[here, :], axis=1, keepdims=True) / (n_tp * cols) + NORM_EPS)
        cosine, sine = cos_ref[here, :], sin_ref[here, :]

        def rotate(v):
            return v * cosine + pltpu.roll(v, KEY_DIM // 2, 1) * sine
        for h in range(heads):
            at = slice(h * KEY_DIM, (h + 1) * KEY_DIM)
            rq[here, at] = rotate(acc_q[here, at] * scale).astype(BF16)
            rk[here, at] = (rotate(acc_k[here, at] * scale) * KEY_DIM ** (-0.5)).astype(BF16)
            m = acc_m[here, at]
            mq[here, at] = (m * lax.rsqrt(jnp.mean(m * m, axis=1, keepdims=True) + NORM_EPS)).astype(BF16)
        rv[here, :] = (acc_v[here, :] * scale).astype(BF16)
        gate[here, :] = jax.nn.sigmoid(acc_g[here, :] * scale)
        return carry

    def retain(c):
        here = pl.ds(c * chunk, chunk)
        start = (c * chunk) // SEQ_LEN * SEQ_LEN
        length = (c + 1) * chunk - start
        whole = pl.ds(start, length)
        t = lax.broadcasted_iota(jnp.int32, (chunk, length), 0) + (c * chunk - start)
        s = lax.broadcasted_iota(jnp.int32, (chunk, length), 1)
        gap = (t - s).astype(F32)
        for h in range(heads):
            at = slice(h * KEY_DIM, (h + 1) * KEY_DIM)
            wide = slice(h * VALUE_DIM, (h + 1) * VALUE_DIM)
            decay = jnp.where(gap >= 0.0, jnp.exp(-rate_ref[h] * jnp.maximum(gap, 0.0)), 0.0)
            scores = dot_nt(rq[here, at], rk[whole, at]) * decay
            upper = scores.astype(BF16)
            lower = (scores - upper.astype(F32)).astype(BF16)
            value = rv[whole, wide]
            o = dot(upper, value) + dot(lower, value)
            o = o - jnp.mean(o, axis=1, keepdims=True)
            ret[here, wide] = o * lax.rsqrt(jnp.mean(o * o, axis=1, keepdims=True) + NORM_EPS)

    def assist(kv, p):
        @pl.when(is_helper)
        def _():
            at = passes.rows(p)
            base = jnp.where(so < 0, CORES, 0)
            kv_out[kv, at, :] = project(at, base, CORES * others, xw[kv]).astype(BF16)
            kv_copy(kv, p).start()

    def attend_keys(n):
        here, there = pl.ds(n * block, block), pl.ds(n * keys, keys)
        state = []
        for h in range(heads):
            at = slice(h * MEM_DIM, (h + 1) * MEM_DIM)
            k = acc_mk[there, at]
            k = (k * lax.rsqrt(jnp.mean(k * k, axis=1, keepdims=True) + NORM_EPS)).astype(BF16)
            exponent = jnp.exp(dot_nt(mq[here, at], k) * MEM_DIM ** (-0.5))
            state.append((exponent.astype(BF16), jnp.sum(exponent, axis=1, keepdims=True)))
        return state

    def attend_values(n, state):
        here, there = pl.ds(n * block, block), pl.ds(n * keys, keys)
        for h in range(heads):
            at = slice(h * MEM_DIM, (h + 1) * MEM_DIM)
            wide = slice(h * VALUE_DIM, (h + 1) * VALUE_DIM)
            exponent, mass = state[h]
            v = acc_mv[there, at].astype(BF16)
            o = (dot(exponent, v) / mass).astype(BF16)
            lifted = dot(o, lift_ref[h])
            out_ref[here, wide] = (ret[here, wide] + gate[here, h:h + 1] * lifted).astype(BF16)

    def attend(n):
        attend_values(n, attend_keys(n))

    def returned(kv, n):
        for p in range(row_pieces):
            if n * keys <= row_cuts[p] < (n + 1) * keys:
                at = passes.rows(p)
                kv_copy(kv, p).wait_recv()
                acc = (acc_mk, acc_mv)[kv]
                acc[at, :] += kv_in[kv, at, :].astype(F32)

    def load_waits():
        for i in range(2, len(pairs)):
            loads[i].wait()

    def settle(c):
        prepare(c, 0)
        retain(c)

    early_parts = min(parts, -(-picks // per))

    def in_tokens(p, distances):
        for d in distances:
            toks.relay(IN, d, p)

    def out_tokens(p):
        for d in outs:
            toks.relay(OUT, d, p)

    def in_rows(p, distances):
        for d in distances:
            passes.relay(IN, d, p)

    def out_rows(p):
        for d in outs:
            passes.relay(OUT, d, p)

    near, far = ins[:1], ins[1:]
    last = blocks - 1

    @pl.when(is_edge)
    def _():
        in_tokens(0, near)
        in_tokens(1, near)
        pass_waits(0, early_parts)
        build(0)
        passes.send_own(0)
        passes.share_own(0)
        for p in range(half + 1, PIECES):
            toks.send_own(p)
        lend_all(others, lent - 1)
        in_tokens(2, near)
        load_waits()
        tokens_of(IN, 0, 0)
        in_tokens(3, near)
        pass_waits(early_parts, parts)
        for n in range(1, blocks):
            build(n)
        for p in range(1, row_pieces):
            passes.send_own(p)
            passes.share_own(p)
            if p == 1:
                lend_all(lent - 1, lent)
        tokens_of(IN, 0, 1)
        in_tokens(0, ins[1:2])
        tokens_of(IN, 1, 0)
        in_tokens(1, ins[1:2])
        tokens_of(IN, 1, 1)
        in_tokens(2, ins[1:2])
        tokens_of(IN, 2, 0)
        in_tokens(3, ins[1:2])
        tokens_of(IN, 2, 1)
        for p in range(row_pieces):
            rows_wait(p, 1)
        for n in range(blocks):
            rows_all(n, z * CORES, CORES)
        for d in ins[2:]:
            in_tokens(0, [d])
            in_tokens(1, [d])
            tokens_of(IN, d, 0)
        settle(0)
        settle(1)
        for d in ins[2:]:
            in_tokens(2, [d])
            in_tokens(3, [d])
            tokens_of(IN, d, 1)
        settle(2)
        settle(3)
        for n in range(blocks):
            returned(0, n)
            state = attend_keys(n)
            returned(1, n)
            attend_values(n, state)
        lend_drain()

    @pl.when(depth > 0)
    def _():
        in_tokens(0, near)
        spread_own(0, 1)
        in_tokens(1, near)
        out_tokens(0)
        in_tokens(2, near)
        spread_own(1, 2)
        pass_waits(0, early_parts)
        build(0)
        passes.send_own(0)
        passes.share_own(0)
        in_tokens(3, near)
        out_tokens(1)
        load_waits()
        tokens_of(IN, 0, 0)
        in_tokens(0, far)
        spread_own(2, others)
        pass_waits(early_parts, parts)
        for n in range(1, blocks):
            build(n)
        for p in range(1, row_pieces):
            passes.share_own(p)
        tokens_of(IN, 0, 1)
        out_tokens(2)
        passes.send_own(1)
        in_rows(0, near)
        tokens_of(IN, 1, 0)
        in_tokens(1, far)
        out_rows(0)
        tokens_of(IN, 1, 1)
        for d in outs:
            tokens_of(OUT, d, 0)
        in_tokens(2, far)
        out_tokens(3)
        passes.send_own(2)
        spread_on(0, others - 1)
        for d in far:
            tokens_of(IN, d, 0)
        spread_on(others - 1, others)
        in_rows(1, near)
        spread_own(others, lent - 2)
        settle(0)
        settle(1)
        spread_own(lent - 2, lent - 1)
        in_rows(0, far)
        rows_wait(0, n_z)
        spread_last(0)
        assist(0, 0)
        in_tokens(3, far)
        out_rows(1)
        for p in range(last, row_pieces):
            passes.send_own(p)
        spread_on(others, lent - 2)
        for d in outs:
            tokens_of(OUT, d, 1)
        in_rows(2, near)
        spread_own(lent - 1, lent)
        spread_on(lent - 2, lent - 1)
        for d in far:
            tokens_of(IN, d, 1)
        out_rows(2)
        in_rows(1, far)
        settle(2)
        spread_on(lent - 1, lent)
        out_rows(3)
        rows_wait(1, n_z)
        assist(0, 1)
        out_rows(4)
        in_rows(last, near)
        spread_last(1)
        assist(1, 0)
        assist(1, 1)
        in_rows(2, far)
        settle(3)
        in_rows(3, far)
        rows_wait(2, n_z)
        assist(0, 2)
        assist(1, 2)
        in_rows(4, near)
        in_rows(4, far)

        def last_returns():
            for p in range(last, row_pieces):
                rows_wait(p, n_z)
                assist(0, p)
                assist(1, p)

        @pl.when(core == 0)
        def _():
            last_returns()
        for n in range(blocks // 2):
            rows_all(n, 0, n_tp)
            attend(n)

        @pl.when(core > 0)
        def _():
            last_returns()
        for n in range(blocks // 2, blocks):
            rows_all(n, 0, n_tp)
            attend(n)

        @pl.when(is_helper)
        def _():
            spread_drain()
            remote(kv_out, kv_in, kv_send.at[0], kv_recv.at[0, 0], st, me_out).wait_send()

    for d in range(1, n_st):
        id_copy(d).wait_send()
    all_slots = slots.at[pl.ds(1, n_st - 1)]
    remote(all_slots, all_slots, pass_send.at[0], pass_recv.at[0], (st + 1) % n_st, me).wait_send()
    toks.drain()
    passes.drain()


def rotary_tables(total):
    half = KEY_DIM // 2
    angle = (np.arange(total) % SEQ_LEN)[:, None] * ROPE_BASE ** (-np.arange(half) / half)[None, :]
    cosine, sine = np.cos(angle), np.sin(angle)
    return (np.concatenate([cosine, cosine], 1).astype(np.float32),
            np.concatenate([-sine, sine], 1).astype(np.float32))


def solution(mesh):
    n_st, n_tp = mesh.shape["st"], mesh.shape["tp"]
    n_z = n_tp // CORES
    assert n_z >= 4

    def per_device(tokens, w_query, w_key, w_value, w_mem_query, w_mem_key, w_mem_value, w_gate, w_lift,
                   decay_rate, store, passage_ids):
        total, cols = tokens.shape
        heads = decay_rate.shape[0]
        blocks, picks = passage_ids.shape
        requests = blocks * picks
        held, pass_rows, _ = store.shape
        cap = max(1, 2 * requests // n_st)
        parts = cap // picks if cap % picks == 0 else 1
        cosine, sine = rotary_tables(total)
        hbm = pl.BlockSpec(memory_space=pl.ANY)
        vmem = pl.BlockSpec(memory_space=pltpu.VMEM)
        smem = pl.BlockSpec(memory_space=pltpu.SMEM)
        V = pltpu.VMEM
        dma = pltpu.SemaphoreType.DMA
        wide = w_value.shape[1]
        key_cols, mem_cols = w_query.shape[1], w_mem_query.shape[1]
        n_b = square_split(n_st)

        row_pieces = len(row_bounds(blocks, picks * pass_rows)) - 1

        def flow_sems(pieces, *pair_shape):
            return dma((n_z, pieces)), dma(pair_shape), dma((n_z,)), dma((1,)), dma((1,))
        all_rows = requests * pass_rows
        scratch = [
            V((n_tp, total, cols), BF16), V((n_tp, all_rows, cols), BF16),
            V(cosine.shape, F32), V(sine.shape, F32), V(w_lift.shape, BF16),
            V(w_query.shape, BF16), V(w_key.shape, BF16), V(w_value.shape, BF16),
            V(w_mem_query.shape, BF16), V(w_mem_key.shape, BF16), V(w_mem_value.shape, BF16),
            V(store.shape, BF16), V((n_st, cap, pass_rows, cols), BF16),
            tuple(V((n_st, cap // parts, pass_rows, cols), BF16) for _ in range(parts)),
            pltpu.SMEM((n_st, picks, blocks), jnp.int32),
            V((total, key_cols), F32), V((total, key_cols), F32), V((total, wide), F32), V((total, mem_cols), F32),
            V((total, heads), F32), V((total, 128), F32),
            V((all_rows, mem_cols), F32), V((all_rows, mem_cols), F32),
            V((total, key_cols), BF16), V((total, key_cols), BF16), V((total, wide), BF16), V((total, mem_cols), BF16),
            V((total, wide), F32), V((total, heads), F32),
            V(w_mem_key.shape, BF16), V(w_mem_value.shape, BF16),
            V((2, all_rows, mem_cols), BF16), V((2, all_rows, mem_cols), BF16),
            dma((13,)), dma((n_st,)), dma((n_st,)), dma((1,)), dma((parts,)),
            flow_sems(PIECES, n_z, 2), flow_sems(row_pieces, row_pieces),
            dma((1,)), dma((2 * (n_z - 1),)), dma((2 * (n_z - 1), n_b - 1)), dma((2 * (n_z - 1), n_st // n_b - 1)),
            dma((2,)), dma((2,)), dma((1,)), dma((2, row_pieces)),
        ]
        return pl.pallas_call(
            functools.partial(kernel, n_st, n_tp, cap, picks, held),
            out_shape=pltpu.VMEM((total, heads * VALUE_DIM), BF16),
            in_specs=[smem] + [hbm] * 7 + [vmem] + [hbm] * 5,
            out_specs=vmem,
            scratch_shapes=scratch,
            compiler_params=pltpu.CompilerParams(
                collective_id=0, has_side_effects=True, vmem_limit_bytes=60 * 1024 * 1024),
        )(decay_rate, tokens, w_query, w_key, w_value, w_mem_query, w_mem_key, w_mem_value,
          w_gate.T, w_lift, jnp.asarray(cosine), jnp.asarray(sine), store, passage_ids.T)

    in_specs = (P("st", "tp"),) + (P(None, "tp"),) * 7 + (
        P("tp", None, None), P("tp"), P("st", None, "tp"), P("st", None))
    return jax.shard_map(per_device, mesh=mesh, in_specs=in_specs, out_specs=P("st", "tp"), check_vma=False)
```
